32 devices in a mesh: sp: 8 (over z, x), tp: 4 (over y, core).
Axes of the slice: x: 2, y: 2, z: 4, core: 2. Of those that a mesh axis runs over, the one named last changes fastest.
Arguments:
- upstream: bfloat16 [2048, 2048], P('sp'), may hold values from -6 to 6
- stream: bfloat16 [2048, 2048], P('sp'), may hold values from -10 to 10
- routes: int32 [2048, 2], P('sp'), may hold values from 0 to 7, all different within a row; in each aligned block of 256 rows (0 to 255, 256 to 511, ...) at most 128 rows name the same one
- route_weights: float32 [2048, 2], P('sp'), may hold values from 0.1 to 1
- glu_value: bfloat16 [2048, 512], P('sp', 'tp'), may hold values from -6 to 6
- glu_gate: bfloat16 [2048, 512], P('sp', 'tp'), may hold values from -10 to 10
- conv_taps: float32 [31, 512], P(None, 'tp'), may hold values from -1 to 1
- conv_saved: bfloat16 [2048, 512], P('sp', 'tp'), may hold values from -600 to 600
- out_proj: bfloat16 [2048, 512], P(None, 'tp'), may hold values from -0.25 to 0.25
- expert_gate: bfloat16 [8, 2048, 2048], P('sp', None, 'tp'), may hold values from -0.125 to 0.125
- expert_up: bfloat16 [8, 2048, 2048], P('sp', None, 'tp'), may hold values from -0.125 to 0.125
- expert_down: bfloat16 [8, 2048, 2048], P('sp', 'tp'), may hold values from -0.125 to 0.125
Outputs:
- grad_stream: bfloat16 [2048, 2048], P('sp', 'tp')
- grad_value: bfloat16 [2048, 512], P('sp', 'tp')
- grad_gate: bfloat16 [2048, 512], P('sp', 'tp')
- grad_out_proj: float32 [2048, 512], P('sp', 'tp')
- grad_expert_gate: float32 [8, 2048, 2048], P('sp', None, 'tp')
- grad_expert_up: float32 [8, 2048, 2048], P('sp', None, 'tp')
- grad_expert_down: float32 [8, 2048, 2048], P('sp', 'tp')
The draws below stay inside these ranges and needn't reach their ends.
Inputs may be any that keep to these rules, and one draw needn't show every extreme that they name: `routes`: each row names 2 different experts; among the 256 rows of one index of sp no expert is named more than 128 times, a bound that some block reaches.
All inputs are finite; a program needn't handle non-finite values.
Results may differ from the reference program's by a relative error of at most 0.014.
Values may be sent and summed in bfloat16 or wider, within the bound.
A program may use at most 128 MiB of HBM per device.

```python
import math
from functools import partial
import jax
import jax.numpy as jnp
import numpy as np
from jax import lax

D = 2048
FF = 2048
CW = 512
KW = 31
TOPK = 2
TOK_DEV = 256
TOKENS = 2048
EXPERTS = 8
CAP = 128
N_SP = 8
N_TP = 4


def draw_conv_saved(key, part):
    key_values, key_rows = jax.random.split(key, 2)
    column_scale = 10.0 ** (jnp.arange(CW, dtype=jnp.float32) / CW)
    values = jnp.clip(jax.random.normal(key_values, (TOKENS, CW), jnp.float32), -4.0, 4.0)
    row_scale = jnp.exp(jax.random.uniform(key_rows, (TOKENS, 1), jnp.float32, 0.0, math.log(10.0)))
    result = values * column_scale[None, :] * row_scale
    return result.astype(jnp.bfloat16)


def raised(drawn, key, source, target, shards_of, factor):
    def block_of(axis_at):
        return (jnp.arange(drawn.shape[axis_at]) // (drawn.shape[axis_at] // shards_of)).reshape((-1,) + (1,) * (drawn.ndim - 1 - axis_at))

    first = jax.random.permutation(key, shards_of)[block_of(target)]
    other_side = (block_of(target) + shards_of // 2) % shards_of
    return jnp.where((block_of(source) == first) | (block_of(source) == other_side), factor * drawn, drawn)


def block_scale(stream_key, shape, pieces, least, largest):
    factor_of, own = 1.0, jax.random.fold_in(stream_key, 6)
    for dim, parts in pieces:
        heights = jnp.exp(jax.random.uniform(jax.random.fold_in(own, dim), (parts,), jnp.float32, least / len(pieces), largest / len(pieces)))
        factor_of = factor_of * jnp.repeat(heights, shape[dim] // parts).reshape([-1 if axis == dim else 1 for axis in range(len(shape))])
    return factor_of


def routed_block(stream_key, own, number, rows, count, top, reach, skew):
    order = jax.random.permutation(stream_key, count)
    packed, usual = load_shares(count, rows * top, reach, skew, True), load_shares(count, rows * top, reach, skew, False)
    places = jnp.arange(count)

    def named(sizes, offset_by):
        used = int((sizes > 0).sum())
        fixed = max(1, used // 4)
        moved = fixed + (places - fixed + offset_by * (used - fixed)) % max(1, count - fixed)
        return jnp.zeros((count,), jnp.int32).at[order[jnp.where(places < fixed, places, moved)]].set(jnp.asarray(sizes, jnp.int32))

    sizes = jnp.where(number % 4 == 0, named(packed, number // 4), named(usual, number - number // 4 - 1))
    mixed = jax.random.permutation(jax.random.fold_in(own, 3), count)
    source_of, receiver = mixed[0:count // 2 * 2:2], mixed[1:count // 2 * 2:2]
    slack = jnp.minimum(sizes[source_of] - 1, reach - sizes[receiver]) // 2
    slack = jnp.where((source_of == order[0]) | (receiver == order[0]) | (sizes[receiver] == 0), 0, jnp.maximum(slack, 0))
    moved = jax.random.randint(jax.random.fold_in(own, 4), (count // 2,), 0, 1 << 20) % (slack + 1)
    sizes = sizes.at[source_of].add(-moved).at[receiver].add(moved)
    items = jnp.searchsorted(jnp.cumsum(sizes), jnp.arange(rows * top), side="right").astype(jnp.int32)
    table = items.reshape(top, rows).T
    table = table[jax.random.permutation(jax.random.fold_in(own, 1), rows)]
    offset_by = jax.random.randint(jax.random.fold_in(own, 2), (rows, 1), 0, top)
    return jnp.take_along_axis(table, (jnp.arange(top)[None, :] + offset_by) % top, axis=1)


def load_shares(amount, total, most, lean, full):
    loads = [(1 << 20) // math.isqrt(standing ** lean) + 1 for standing in range(1, amount + 1)]
    largest = most if full else min(most, max(-(-total // amount), total * loads[0] // sum(loads)))
    least = 1 if total - largest >= amount - 1 else 0
    given, surplus = [largest] + [least] * (amount - 1), total - largest - least * (amount - 1)
    while surplus > 0:
        free = [i for i in range(1, amount) if given[i] < largest] or [i for i in range(1, amount) if given[i] < most]
        mass, left = sum([loads[i] for i in free]), surplus
        for i in free:
            more = min(most - given[i], max(1, left * loads[i] // mass), surplus)
            given[i] = given[i] + more
            surplus = surplus - more
    return np.array(given)


def bell_draw(rng, extent, deviation, limit, cuts=(), kind=jnp.bfloat16):
    entries = jax.random.normal(rng, extent, jnp.float32) * deviation
    if len(cuts) > 0:
        entries = block_scale(rng, extent, cuts, -0.22, 0.18) * entries
    return jnp.clip(entries, min=-limit, max=limit).astype(kind)


def heavy_noise(stream_key, shape, scale, most, cuts, heavy, kind=jnp.bfloat16):
    array = scale * jax.random.normal(stream_key, shape, jnp.float32)
    if cuts:
        array = array * block_scale(stream_key, shape, cuts, -0.22, 0.18)
    return jnp.clip(raised(array, jax.random.fold_in(stream_key, 3), *heavy), -most, most).astype(kind)


def setup_inputs(seed: int = 0) -> dict:
    seeds = jax.random.split(jax.random.key(seed), 13)
    upstream = heavy_noise(seeds[0], (TOKENS, D), 1.0, 6.0, ((0, 8),), (0, 1, 8, 2.0))
    stream = bell_draw(seeds[1], (TOKENS, D), 1.0, 10.0, ((0, 8),))
    routes_keys = jax.random.split(jax.random.fold_in(seeds[2], 1), TOKENS // TOK_DEV)
    routes_turns = jax.random.permutation(jax.random.fold_in(seeds[2], 3), TOKENS // TOK_DEV)
    routes = jax.vmap(lambda own, number: routed_block(jax.random.fold_in(seeds[2], 2), own, number, TOK_DEV, EXPERTS, TOPK, CAP, 2))(routes_keys, routes_turns).reshape((TOKENS, TOPK))
    route_weights = jnp.clip(0.1 + 0.9 * jax.random.uniform(seeds[3], (TOKENS, TOPK), jnp.float32) ** block_scale(seeds[3], (TOKENS, TOPK), ((0, 8),), -0.2, 0.2), 0.1, 1.0)
    glu_value = bell_draw(seeds[4], (TOKENS, CW), 1.0, 6.0, ((0, 8), (1, 4)))
    glu_gate = bell_draw(seeds[5], (TOKENS, CW), 2.0, 10.0, ((0, 8), (1, 4)))
    conv_taps = bell_draw(seeds[6], (KW, CW), KW ** -0.5, 1.0, ((1, 4),), jnp.float32)
    conv_saved = draw_conv_saved(jax.random.fold_in(seeds[12], 71), 0)
    out_proj = bell_draw(seeds[8], (D, CW), CW ** -0.5, 0.25, ((1, 4),))
    expert_gate = bell_draw(seeds[9], (EXPERTS, D, FF), D ** -0.5, 0.125, ((0, 8), (2, 4)))
    expert_up = bell_draw(seeds[10], (EXPERTS, D, FF), D ** -0.5, 0.125, ((0, 8), (2, 4)))
    expert_down = bell_draw(seeds[11], (EXPERTS, FF, D), FF ** -0.5, 0.125, ((0, 8), (1, 4)))
    return {"upstream": upstream, "stream": stream, "routes": routes, "route_weights": route_weights, "glu_value": glu_value, "glu_gate": glu_gate, "conv_taps": conv_taps, "conv_saved": conv_saved, "out_proj": out_proj, "expert_gate": expert_gate, "expert_up": expert_up, "expert_down": expert_down}


clamp_limit = 7.0
glu_alpha = 1.702
norm_eps = 1e-05

def contract_rows(left, right):
    return lax.dot_general(left, right, (((0,), (0,)), ((), ())), preferred_element_type=jnp.float32)

def times_transposed(left, right):
    return lax.dot_general(left, right, (((1,), (1,)), ((), ())), preferred_element_type=jnp.float32)

def block_slots(block_routes, expert_count, capacity):
    flat_routes = block_routes.reshape(-1).astype(jnp.int32)
    one_hot = (flat_routes[:, None] == jnp.arange(expert_count, dtype=jnp.int32)[None, :]).astype(jnp.int32)
    earlier = jnp.cumsum(one_hot, axis=0) - one_hot
    slot_index = lax.optimization_barrier(jnp.sum(earlier * one_hot, axis=1)).astype(jnp.int32)
    target = (flat_routes * capacity + slot_index).astype(jnp.int32)
    pair_count = flat_routes.shape[0]
    table = jnp.full((expert_count * capacity,), pair_count, jnp.int32).at[target].set(jnp.arange(pair_count, dtype=jnp.int32))
    return (target, table)

def gather_pairs(table, block_stream, block_upstream, block_weights, topk):
    token_of = table // topk
    zero_row = jnp.zeros((1, block_stream.shape[1]), jnp.bfloat16)
    stream_pad = jnp.concatenate([block_stream, zero_row], axis=0)
    upstream_pad = jnp.concatenate([block_upstream, zero_row], axis=0)
    weight_pad = jnp.concatenate([block_weights.reshape(-1), jnp.zeros((1,), jnp.float32)])
    send_rows = stream_pad[token_of]
    send_cot = (weight_pad[table][:, None] * upstream_pad[token_of].astype(jnp.float32)).astype(jnp.bfloat16)
    return (send_rows, send_cot)

def expert_backward(expert_rows, expert_cot, gate_weight, up_weight, down_weight):
    gate_pre = jnp.dot(expert_rows, gate_weight, preferred_element_type=jnp.float32)
    up_pre = jnp.dot(expert_rows, up_weight, preferred_element_type=jnp.float32)
    capped = jnp.minimum(gate_pre, clamp_limit)
    clipped = jnp.clip(up_pre, -clamp_limit, clamp_limit)
    gate_sigmoid = jax.nn.sigmoid(glu_alpha * capped)
    act = (capped * gate_sigmoid * (clipped + 1.0)).astype(jnp.bfloat16)
    grad_down = contract_rows(act, expert_cot)
    grad_act = times_transposed(expert_cot, down_weight)
    slope = gate_sigmoid + glu_alpha * capped * gate_sigmoid * (1.0 - gate_sigmoid)
    grad_gate_pre = jnp.where(gate_pre < clamp_limit, grad_act * (clipped + 1.0) * slope, 0.0).astype(jnp.bfloat16)
    grad_up_pre = jnp.where(jnp.abs(up_pre) < clamp_limit, grad_act * capped * gate_sigmoid, 0.0).astype(jnp.bfloat16)
    grad_gate = contract_rows(expert_rows, grad_gate_pre)
    grad_up = contract_rows(expert_rows, grad_up_pre)
    return (grad_gate, grad_up, grad_down, grad_gate_pre, grad_up_pre)

def one_expert(operands):
    expert_rows, expert_cot, gate_weight, up_weight, down_weight = operands
    grad_gate, grad_up, grad_down, grad_gate_pre, grad_up_pre = expert_backward(expert_rows, expert_cot, gate_weight, up_weight, down_weight)
    group_width = FF // N_TP
    gate_groups = grad_gate_pre.astype(jnp.float32).reshape(-1, N_TP, group_width)
    up_groups = grad_up_pre.astype(jnp.float32).reshape(-1, N_TP, group_width)
    gate_split = gate_weight.astype(jnp.float32).reshape(D, N_TP, group_width)
    up_split = up_weight.astype(jnp.float32).reshape(D, N_TP, group_width)
    partial_rows = jnp.einsum('rgf,dgf->grd', gate_groups, gate_split) + jnp.einsum('rgf,dgf->grd', up_groups, up_split)
    rounded = lax.optimization_barrier(partial_rows.astype(jnp.bfloat16))
    row_grad = lax.optimization_barrier(jnp.sum(rounded.astype(jnp.float32), axis=0)).astype(jnp.bfloat16)
    return (grad_gate, grad_up, grad_down, row_grad)

def take_rows(source_rows, target_rows):
    return source_rows[target_rows]

def reference(upstream, stream, routes, route_weights, glu_value, glu_gate, conv_taps, conv_saved, out_proj, expert_gate, expert_up, expert_down):
    block_routes = routes.reshape(N_SP, TOK_DEV, TOPK)
    targets, tables = jax.vmap(partial(block_slots, expert_count=EXPERTS, capacity=CAP))(block_routes)
    send_rows, send_cot = jax.vmap(partial(gather_pairs, topk=TOPK))(tables, stream.reshape(N_SP, TOK_DEV, D), upstream.reshape(N_SP, TOK_DEV, D), route_weights.reshape(N_SP, TOK_DEV, TOPK))
    expert_rows = send_rows.reshape(N_SP, EXPERTS, CAP, D).transpose(1, 0, 2, 3).reshape(EXPERTS, N_SP * CAP, D)
    expert_cot = send_cot.reshape(N_SP, EXPERTS, CAP, D).transpose(1, 0, 2, 3).reshape(EXPERTS, N_SP * CAP, D)
    grad_expert_gate, grad_expert_up, grad_expert_down, row_grads = lax.map(one_expert, (expert_rows, expert_cot, expert_gate, expert_up, expert_down))
    returned = row_grads.reshape(EXPERTS, N_SP, CAP, D).transpose(1, 0, 2, 3).reshape(N_SP, EXPERTS * CAP, D)
    pair_grads = jax.vmap(take_rows)(returned, targets)
    routed_sum = lax.optimization_barrier(jnp.sum(pair_grads.astype(jnp.float32).reshape(TOKENS, TOPK, D), axis=1))
    grad_stream = (upstream.astype(jnp.float32) + routed_sum).astype(jnp.bfloat16)
    saved_conv = conv_saved.astype(jnp.float32)
    mean_c = lax.optimization_barrier(jnp.mean(saved_conv, axis=1, keepdims=True))
    var_c = lax.optimization_barrier(jnp.mean(saved_conv * saved_conv, axis=1, keepdims=True)) - mean_c * mean_c
    inv_std = lax.rsqrt(var_c + norm_eps)
    normed = (saved_conv - mean_c) * inv_std
    norm_sigmoid = jax.nn.sigmoid(normed)
    mixed = (normed * norm_sigmoid).astype(jnp.bfloat16)
    grad_mixed = jnp.dot(grad_stream, out_proj, preferred_element_type=jnp.float32)
    grad_normed = grad_mixed * norm_sigmoid * (1.0 + normed * (1.0 - norm_sigmoid))
    first_mean = lax.optimization_barrier(jnp.mean(grad_normed, axis=1, keepdims=True))
    second_mean = lax.optimization_barrier(jnp.mean(grad_normed * normed, axis=1, keepdims=True))
    grad_conv = inv_std * (grad_normed - first_mean - normed * second_mean)
    padded = jnp.concatenate([grad_conv, jnp.zeros((KW - 1, CW), jnp.float32)], axis=0)
    grad_glu = jnp.zeros((TOKENS, CW), jnp.float32)
    for offset in range(KW):
        grad_glu = grad_glu + conv_taps[offset][None, :] * padded[offset:offset + TOKENS]
    gate_sig = jax.nn.sigmoid(glu_gate.astype(jnp.float32))
    grad_value = (grad_glu * gate_sig).astype(jnp.bfloat16)
    grad_gate = (grad_glu * glu_value.astype(jnp.float32) * gate_sig * (1.0 - gate_sig)).astype(jnp.bfloat16)
    grad_out_proj = contract_rows(grad_stream, mixed)
    return (grad_stream, grad_value, grad_gate, grad_out_proj, grad_expert_gate, grad_expert_up, grad_expert_down)
```

```python
import functools

import jax
import jax.numpy as jnp
from jax import lax
from jax.experimental import pallas as pl
from jax.experimental.pallas import tpu as pltpu
from jax.sharding import PartitionSpec as P


clamp_limit = 7.0
glu_alpha = 1.702
norm_eps = 1e-05


def contract_rows(left, right):
    return lax.dot_general(
        left, right, (((0,), (0,)), ((), ())), preferred_element_type=jnp.float32
    )


def times_transposed(left, right):
    return lax.dot_general(
        left, right, (((1,), (1,)), ((), ())), preferred_element_type=jnp.float32
    )


def greet(sp_count, tp_count):
    me, lane = lax.axis_index("sp"), lax.axis_index("tp")
    barrier = pltpu.get_barrier_semaphore()
    for step in range(1, sp_count):
        pl.semaphore_signal(
            barrier,
            inc=1,
            device_id={"sp": lax.rem(me + step, sp_count)},
            device_id_type=pl.DeviceIdType.MESH,
        )
    for step in range(1, tp_count):
        pl.semaphore_signal(
            barrier,
            inc=1,
            device_id={"tp": lax.rem(lane + step, tp_count)},
            device_id_type=pl.DeviceIdType.MESH,
        )
    pl.semaphore_wait(barrier, sp_count + tp_count - 2)


def remote(src, dst, send_sem, recv_sem, **target):
    return pltpu.make_async_remote_copy(
        src_ref=src,
        dst_ref=dst,
        send_sem=send_sem,
        recv_sem=recv_sem,
        device_id=target,
        device_id_type=pl.DeviceIdType.MESH,
    )


def load_in(src, dst, sem):
    return pltpu.make_async_copy(src, dst, sem)


def fused_kernel(
    sp_count,
    tp_count,
    meta_ref,
    stream_hbm,
    upstream_hbm,
    gate_hbm,
    up_hbm,
    down_hbm,
    saved_hbm,
    proj_hbm,
    taps_hbm,
    value_hbm,
    conv_gate_hbm,
    grad_stream_ref,
    grad_value_ref,
    grad_gate_ref,
    grad_proj_ref,
    gate_out,
    up_out,
    down_out,
    tokens,
    weights,
    down_ref,
    saved_ref,
    proj_ref,
    taps_ref,
    value_ref,
    gate_ref,
    metas,
    chained,
    both,
    chosen,
    gains,
    near_out,
    cross_out,
    before,
    picks_all,
    picks_t,
    act_t,
    slopes,
    partial,
    pair_in,
    side_out,
    side_in,
    total,
    returned,
    full,
    stat_out,
    stat_in,
    parts_out,
    parts_in,
    rim_in,
    padded,
    gate_acc,
    up_acc,
    down_acc,
    load_sem,
    store_sem,
    meta_send,
    meta_recv,
    chain_send,
    chain_recv,
    cross_send,
    cross_recv,
    along_send,
    along_recv,
    twin_send,
    twin_recv,
    pair_send,
    pair_recv,
    side_send,
    side_recv,
    far_send,
    far_recv,
    full_send,
    full_recv,
    stat_send,
    stat_recv,
    parts_send,
    parts_recv,
    rim_send,
    rim_recv,
):
    me, lane = lax.axis_index("sp"), lax.axis_index("tp")
    chips = tp_count // 2
    across = chips
    layers = sp_count // across
    layer, place = lax.div(me, across), lax.rem(me, across)
    core = lax.rem(lane, 2)
    partner = lane + 1 - 2 * core
    tok_count, model_width = tokens.shape[1:]
    capacity = both.shape[2]
    width = model_width // tp_count
    hidden = down_ref.shape[0]
    group_rows = across * capacity
    channels = saved_ref.shape[1]
    conv_width = channels * tp_count
    groups = tok_count // 128
    f32, bf16 = jnp.float32, jnp.bfloat16

    loads = [
        load_in(stream_hbm, tokens.at[0], load_sem.at[0]),
        load_in(upstream_hbm, tokens.at[1], load_sem.at[1]),
        load_in(saved_hbm, saved_ref, load_sem.at[2]),
        load_in(gate_hbm.at[0], weights.at[:, pl.ds(0, hidden)], load_sem.at[3]),
        load_in(up_hbm.at[0], weights.at[:, pl.ds(hidden, hidden)], load_sem.at[4]),
        load_in(down_hbm.at[0], down_ref, load_sem.at[5]),
        load_in(proj_hbm, proj_ref, load_sem.at[6]),
        load_in(taps_hbm, taps_ref, load_sem.at[7]),
        load_in(value_hbm, value_ref, load_sem.at[8]),
        load_in(conv_gate_hbm, gate_ref, load_sem.at[9]),
    ]
    for load in loads:
        load.start()

    before[...] = jnp.where(
        lax.broadcasted_iota(jnp.int32, before.shape, 0)
        < lax.broadcasted_iota(jnp.int32, before.shape, 1),
        1.0,
        0.0,
    ).astype(bf16)

    greet(sp_count, tp_count)
    started = []

    def begin(copy):
        copy.start()
        started.append(copy)

    def columns(column):
        return pl.ds(pl.multiple_of(column * width, width), width)

    def layer_at(step):
        if step == 0:
            return layer
        inner = jnp.minimum(layer, layers - 1 - layer)
        paired = step <= 2 * inner
        reach = jnp.where(paired, (step + 1) // 2, step - inner)
        below = jnp.where(paired, step % 2 == 1, layer > layers - 1 - layer)
        return jnp.where(below, layer - reach, layer + reach)

    at_layer = [layer_at(step) for step in range(layers)]

    def block_at(step, index):
        return at_layer[step] * across + lax.rem(place + across - index, across)

    def give_meta(step):
        return remote(
            meta_ref,
            metas.at[layer],
            meta_send.at[step],
            meta_recv.at[layer],
            sp=lax.rem(me + step * across, sp_count),
        )

    for step in range(1, layers):
        begin(give_meta(step))

    def own_chain(which, up):
        to = me + across if up else me + sp_count - across
        return remote(
            tokens.at[which, :, columns(lane)],
            chained.at[which, layer],
            chain_send.at[which, 0, int(up)],
            chain_recv.at[which, layer],
            sp=lax.rem(to, sp_count),
        )

    def chain_on(which, step):
        source = at_layer[step]
        to = jnp.where(source < layer, me + across, me + sp_count - across)
        return remote(
            chained.at[which, source],
            chained.at[which, source],
            chain_send.at[which, step, 0],
            chain_recv.at[which, source],
            sp=lax.rem(to, sp_count),
        )

    def goes_on(step):
        source = at_layer[step]
        return jnp.where(source < layer, layer < layers - 1, layer > 0)

    for which in range(2):
        loads[which].wait()

        @pl.when(layer < layers - 1)
        def _():
            own_chain(which, True).start()

        @pl.when(layer > 0)
        def _():
            own_chain(which, False).start()

    def piece(which, block, column):
        return both.at[which, block, :, columns(column)]

    def column_at(hop):
        return lax.rem(lane + tp_count - 2 * hop, tp_count)

    def cross(which, step, index, hop):
        column = column_at(hop)
        source = near_out.at[which, index - 1, hop] if step == 0 else cross_out.at[which, step - 1, index - 1]
        return remote(
            source,
            piece(which, block_at(step, 0), column),
            cross_send.at[which, step, index - 1, hop],
            cross_recv.at[which, step, index - 1, hop],
            sp=layer * across + lax.rem(place + index, across),
        )

    def along(which, step, index, hop):
        here = piece(which, block_at(step, index), lane)
        return remote(
            here,
            here,
            along_send.at[which, step, index, hop - 1],
            along_recv.at[which, step, index, hop - 1],
            tp=lax.rem(lane + 2 * hop, tp_count),
        )

    def twin(which, step, index, hop):
        here = piece(which, block_at(step, index), column_at(hop))
        return remote(
            here,
            here,
            twin_send.at[which, step, index, hop],
            twin_recv.at[which, step, index, hop],
            tp=partner,
        )

    def choose(meta):
        rows = lax.broadcasted_iota(jnp.int32, (8, tok_count), 0) + place
        rows = jnp.where(rows >= across, rows - across, rows) + layer * across
        names = rows.astype(f32)
        hit = jnp.where((meta[0:1] == names) | (meta[1:2] == names), 1.0, 0.0)
        slots = jnp.dot(hit.astype(bf16), before[...], preferred_element_type=f32)
        slot_rows = lax.broadcasted_iota(jnp.int32, (capacity, tok_count), 0).astype(f32)
        for index in range(across):
            pick = jnp.where(
                (slots[index : index + 1] == slot_rows) & (hit[index : index + 1] > 0.0), 1.0, 0.0
            )
            chosen[index] = pick.astype(bf16)
            gain = jnp.where(meta[0:1] == names[index : index + 1], meta[2:3], meta[3:4])
            row_gain = jnp.sum(pick * gain, axis=1, keepdims=True)
            gains[index] = jnp.broadcast_to(row_gain, (capacity, 128))

    def picked(which, index, source):
        rows = jnp.dot(chosen[index], source, preferred_element_type=f32)
        if which == 1:
            rows = rows * gains[index][:, :1]
        return rows.astype(bf16)

    def stage_forward(step):
        @pl.when(goes_on(step))
        def _():
            for which in range(2):
                chain_on(which, step).wait_recv()
                chain_on(which, step).start()

    def stage_select(step):
        if step == 0:
            choose(meta_ref[...])
            for which in range(2):
                for index in range(1, across):
                    for hop in range(chips):
                        near_out[which, index - 1, hop] = picked(
                            which, index, tokens[which, :, columns(column_at(hop))]
                        )
                        begin(cross(which, 0, index, hop))
            for which in range(2):
                for column in range(tp_count):
                    both[which, me, :, column * width : (column + 1) * width] = picked(
                        which, 0, tokens[which, :, column * width : (column + 1) * width]
                    )
            return
        source = at_layer[step]
        remote(
            meta_ref, metas.at[source], meta_send.at[0], meta_recv.at[source], sp=lax.rem(me + across, sp_count)
        ).wait_recv()
        choose(metas[source])
        for which in range(2):

            @pl.when(jnp.logical_not(goes_on(step)))
            def _():
                chain_on(which, step).wait_recv()

            for index in range(1, across):
                cross_out[which, step - 1, index - 1] = picked(which, index, chained[which, source])
                begin(cross(which, step, index, 0))
            both[which, block_at(step, 0), :, columns(lane)] = picked(which, 0, chained[which, source])
            for hop in range(1, chips):
                begin(along(which, step, 0, hop))
            begin(twin(which, step, 0, 0))

    def stage_cross(step):
        for which in range(2):
            for index in range(1, across):
                for hop in range(chips if step == 0 else 1):
                    cross(which, step, index, hop).wait_recv()
                    if step:
                        for side in range(1, chips):
                            begin(along(which, step, index, side))
                    begin(twin(which, step, index, hop))

    def stage_along(step):
        if step == 0:
            return
        for which in range(2):
            for index in range(across):
                for hop in range(1, chips):
                    along(which, step, index, hop).wait_recv()
                    begin(twin(which, step, index, hop))

    def group_at(step):
        return pl.ds(at_layer[step] * across, across)

    hidden_tile = min(hidden, 256)

    def stage_expert(step):
        for which in range(2):
            for index in range(across):
                if step or index:
                    for hop in range(chips):
                        twin(which, step, index, hop).wait_recv()
        if step == 0:
            for load in loads[3:6]:
                load.wait()
        first = pl.multiple_of(at_layer[step] * group_rows, group_rows)
        rows_at = pl.ds(first, group_rows)

        @pl.loop(0, hidden // hidden_tile)
        def _(tile):
            units = pl.ds(pl.multiple_of(tile * hidden_tile, hidden_tile), hidden_tile)
            up_units = pl.ds(pl.multiple_of(hidden + tile * hidden_tile, hidden_tile), hidden_tile)
            rows = both[0, group_at(step)].reshape(group_rows, model_width)
            cot = both[1, group_at(step)].reshape(group_rows, model_width)
            gate_pre = jnp.dot(rows, weights[:, units], preferred_element_type=f32)
            up_pre = jnp.dot(rows, weights[:, up_units], preferred_element_type=f32)
            grad_act = times_transposed(cot, down_ref[units, :])
            capped = jnp.minimum(gate_pre, clamp_limit)
            clipped = jnp.clip(up_pre, -clamp_limit, clamp_limit)
            sig = jax.nn.sigmoid(glu_alpha * capped)
            gated = capped * sig
            act_t[units, rows_at] = (gated * (clipped + 1.0)).T.astype(bf16)
            slope = sig + glu_alpha * gated * (1.0 - sig)
            slopes[rows_at, units] = jnp.where(
                gate_pre < clamp_limit, grad_act * (clipped + 1.0) * slope, 0.0
            ).astype(bf16)
            slopes[rows_at, up_units] = jnp.where(
                jnp.abs(up_pre) < clamp_limit, grad_act * gated, 0.0
            ).astype(bf16)

        @pl.loop(0, tp_count)
        def _(tile):
            value = times_transposed(slopes[rows_at, :], weights[columns(tile), :])
            partial[group_at(step), :, columns(tile)] = value.astype(bf16).reshape(
                across, capacity, width
            )

        for hop in list(range(1, chips)) + [0]:
            begin(swapped(step, hop))

    def swapped(step, hop):
        other = lax.rem(lane + 2 * hop, tp_count) + 1 - 2 * core
        return remote(
            partial.at[group_at(step), :, columns(other)],
            pair_in.at[step, hop],
            pair_send.at[step, hop],
            pair_recv.at[step, hop],
            tp=partner,
        )

    def beside(step, hop):
        return remote(
            side_out.at[step, hop - 1],
            side_in.at[step, hop - 1],
            side_send.at[step, hop - 1],
            side_recv.at[step, hop - 1],
            tp=lax.rem(lane + 2 * hop, tp_count),
        )

    def pair_sum(step, hop):
        column = lax.rem(lane + 2 * hop, tp_count)
        return partial[group_at(step), :, columns(column)].astype(f32) + pair_in[step, hop].astype(f32)

    def stage_pair(step):
        for hop in range(1, chips):
            swapped(step, hop).wait_recv()
            side_out[step, hop - 1] = pair_sum(step, hop).astype(bf16)
            begin(beside(step, hop))

    def stage_return(step):
        swapped(step, 0).wait_recv()
        value = pair_sum(step, 0)
        for hop in range(1, chips):
            beside(step, hop).wait_recv()
            value += side_in[step, hop - 1].astype(f32)
        total[step] = value.astype(bf16)
        for index in range(across):
            spot = lax.rem(place + index, across)
            if step == 0 and index == 0:
                returned[me] = total[0, spot]
            else:
                begin(
                    remote(
                        total.at[step, spot],
                        returned.at[me],
                        far_send.at[step, index],
                        far_recv.at[me],
                        sp=at_layer[step] * across + spot,
                    )
                )

    stage_select(0)

    eye = (
        lax.broadcasted_iota(jnp.int32, (128, 128), 0)
        == lax.broadcasted_iota(jnp.int32, (128, 128), 1)
    )

    def stat(phase, hop):
        return remote(
            stat_out.at[phase],
            stat_in.at[phase, hop],
            stat_send.at[phase, hop],
            stat_recv.at[phase, hop],
            tp=lax.rem(lane + hop, tp_count),
        )

    def share(phase, sums):
        stat_out[phase] = jnp.zeros(stat_out.shape[1:], f32)
        row = 0
        for item in sums:
            for group in range(groups):
                part = item[group * 128 : (group + 1) * 128]
                spread = jnp.where(eye, jnp.broadcast_to(part, (128, 128)), 0.0)
                stat_out[phase, row : row + 1] = jnp.sum(spread, axis=0, keepdims=True)
                row += 1
        for hop in range(1, tp_count):
            begin(stat(phase, hop))

    def shared(phase):
        value = stat_out[phase]
        for hop in range(1, tp_count):
            stat(phase, hop).wait_recv()
            value += stat_in[phase, hop]
        columns_of = []
        for item in range(2):
            parts = []
            for group in range(groups):
                row = item * groups + group
                spread = jnp.broadcast_to(value[row : row + 1], (128, 128))
                parts.append(jnp.sum(jnp.where(eye, spread, 0.0), axis=1, keepdims=True))
            columns_of.append(jnp.concatenate(parts, axis=0))
        return columns_of

    loads[2].wait()
    first_conv = saved_ref[...].astype(f32)
    share(
        0,
        (
            jnp.sum(first_conv, axis=1, keepdims=True),
            jnp.sum(first_conv * first_conv, axis=1, keepdims=True),
        ),
    )

    own_meta = meta_ref[...]
    names = lax.broadcasted_iota(jnp.int32, (sp_count, tok_count), 0).astype(f32)
    hit = jnp.where((own_meta[0:1] == names) | (own_meta[1:2] == names), 1.0, 0.0)
    slots = jnp.dot(hit.astype(bf16), before[...], preferred_element_type=f32)
    slot_rows = lax.broadcasted_iota(jnp.int32, (capacity, tok_count), 0).astype(f32)
    for expert in range(sp_count):
        pick = jnp.where(
            (slots[expert : expert + 1] == slot_rows) & (hit[expert : expert + 1] > 0.0), 1.0, 0.0
        )
        picks_all[expert * capacity : (expert + 1) * capacity] = pick.astype(bf16)
    picks_t[...] = picks_all[...].astype(f32).T.astype(bf16)

    if layers > 1:
        stage_forward(1)
        stage_select(1)
    if layers > 2:
        stage_forward(2)
    stage_cross(0)
    stage_expert(0)
    stage_pair(0)
    for step in range(2, layers + 1):
        stage_cross(step - 1)
        if step < layers:
            stage_select(step)
        if step + 1 < layers:
            stage_forward(step + 1)
        stage_along(step - 1)
        stage_expert(step - 1)
        stage_return(step - 2)
        stage_pair(step - 1)

    tile_width = 256
    tiles = model_width // tile_width
    rows_total = sp_count * capacity

    def down_store(tile):
        at = pl.ds(pl.multiple_of(tile * tile_width, tile_width), tile_width)
        return pltpu.make_async_copy(down_acc.at[:, at], down_out.at[0, :, at], store_sem.at[0, tile])

    def gate_store(tile):
        at = pl.ds(pl.multiple_of(tile * tile_width, tile_width), tile_width)
        return pltpu.make_async_copy(gate_acc.at[at], gate_out.at[0, at], store_sem.at[1, tile])

    def up_store(tile):
        at = pl.ds(pl.multiple_of(tile * tile_width, tile_width), tile_width)
        return pltpu.make_async_copy(up_acc.at[at], up_out.at[0, at], store_sem.at[2, tile])

    @pl.loop(0, tiles)
    def _(tile):
        at = pl.ds(pl.multiple_of(tile * tile_width, tile_width), tile_width)
        down_acc[:, at] = jnp.dot(
            act_t[...], both[1, :, :, at].reshape(rows_total, tile_width), preferred_element_type=f32
        )
        down_store(tile).start()

    stage_return(layers - 1)

    @pl.loop(0, tiles)
    def _(tile):
        at = pl.ds(pl.multiple_of(tile * tile_width, tile_width), tile_width)
        left = both[0, :, :, at].reshape(rows_total, tile_width)
        gate_acc[at] = contract_rows(left, slopes[:, :hidden])
        up_acc[at] = contract_rows(left, slopes[:, hidden:])
        gate_store(tile).start()
        up_store(tile).start()

    total_sum, square_sum = shared(0)
    mean_c = total_sum / conv_width
    var_c = square_sum / conv_width - mean_c * mean_c
    inv_std = lax.rsqrt(var_c + norm_eps)
    saved_conv = saved_ref[...].astype(f32)
    normed = (saved_conv - mean_c) * inv_std
    norm_sigmoid = jax.nn.sigmoid(normed)
    mixed = (normed * norm_sigmoid).astype(bf16)
    for load in loads[6:]:
        load.wait()

    for step in range(1, sp_count):
        source = lax.rem(me + step, sp_count)
        remote(
            total.at[0, 0], returned.at[source], far_send.at[0, 0], far_recv.at[source], sp=source
        ).wait_recv()
    routed_sum = jnp.dot(
        picks_t[...],
        returned[...].reshape(-1, width),
        preferred_element_type=f32,
    )
    own_grad = (tokens[1, :, columns(lane)].astype(f32) + routed_sum).astype(bf16)
    grad_stream_ref[...] = own_grad
    full[:, columns(lane)] = own_grad

    def spread_full(hop):
        return remote(
            full.at[:, columns(lane)],
            full.at[:, columns(lane)],
            full_send.at[0, hop],
            full_recv.at[0, hop],
            tp=lax.rem(lane + 2 * hop, tp_count),
        )

    def hand_over(hop):
        column = lax.rem(lane + tp_count - 2 * hop, tp_count)
        return remote(
            full.at[:, columns(column)],
            full.at[:, columns(column)],
            full_send.at[1, hop],
            full_recv.at[1, hop],
            tp=partner,
        )

    for hop in range(1, chips):
        begin(spread_full(hop))
    begin(hand_over(0))
    for hop in range(1, chips):
        spread_full(hop).wait_recv()
        begin(hand_over(hop))
    for hop in range(chips):
        hand_over(hop).wait_recv()

    for column in range(tp_count):
        block = contract_rows(full[:, column * width : (column + 1) * width], mixed)
        per = sp_count // tp_count
        parts_out[column * per : (column + 1) * per] = block.reshape(
            per, width // per, channels
        ).astype(bf16)

    def give_parts(step):
        to = lax.rem(me + step, sp_count)
        return remote(
            parts_out.at[to],
            parts_in.at[step],
            parts_send.at[step],
            parts_recv.at[step],
            sp=to,
        )

    for step in range(1, sp_count):
        begin(give_parts(step))

    grad_mixed = jnp.dot(full[...], proj_ref[...], preferred_element_type=f32)
    grad_normed = grad_mixed * norm_sigmoid * (1.0 + normed * (1.0 - norm_sigmoid))
    share(
        1,
        (
            jnp.sum(grad_normed, axis=1, keepdims=True),
            jnp.sum(grad_normed * normed, axis=1, keepdims=True),
        ),
    )
    first_sum, second_sum = shared(1)
    grad_conv = inv_std * (
        grad_normed - first_sum / conv_width - normed * (second_sum / conv_width)
    )
    padded[:tok_count] = grad_conv
    rim = rim_in.shape[0]
    rim_copy = remote(
        padded.at[pl.ds(0, rim)],
        rim_in,
        rim_send.at[0],
        rim_recv.at[0],
        sp=lax.rem(me + sp_count - 1, sp_count),
    )
    begin(rim_copy)
    gate_sig = jax.nn.sigmoid(gate_ref[...].astype(f32))
    rim_copy.wait_recv()
    padded[tok_count:] = jnp.where(me == sp_count - 1, 0.0, rim_in[...])
    grad_glu = jnp.zeros((tok_count, channels), f32)
    for offset in range(taps_ref.shape[0]):
        grad_glu += taps_ref[offset : offset + 1] * padded[offset : offset + tok_count]
    grad_value_ref[...] = (grad_glu * gate_sig).astype(bf16)
    grad_gate_ref[...] = (
        grad_glu * value_ref[...].astype(f32) * gate_sig * (1.0 - gate_sig)
    ).astype(bf16)

    summed = parts_out[me].astype(f32)
    for step in range(1, sp_count):
        give_parts(step).wait_recv()
        summed += parts_in[step].astype(f32)
    grad_proj_ref[...] = summed

    @pl.loop(0, tiles)
    def _(tile):
        down_store(tile).wait()
        gate_store(tile).wait()
        up_store(tile).wait()

    for copy in started:
        copy.wait_send()
    for which in range(2):

        @pl.when(layer < layers - 1)
        def _():
            own_chain(which, True).wait_send()

        @pl.when(layer > 0)
        def _():
            own_chain(which, False).wait_send()

        for step in range(1, layers):

            @pl.when(goes_on(step))
            def _():
                chain_on(which, step).wait_send()


def fused(sp_count, tp_count, capacity, meta, stream, upstream, gate_w, up_w, down_w, *conv_args):
    conv_saved, out_proj, conv_taps = conv_args[:3]
    tok_count, model_width = stream.shape
    channels = conv_saved.shape[1]
    hidden = down_w.shape[1]
    width = model_width // tp_count
    chips = tp_count // 2
    across = chips
    layers = sp_count // across
    rim = -(-(conv_taps.shape[0] - 1) // 8) * 8
    dma, vmem = pltpu.SemaphoreType.DMA, pltpu.VMEM
    f32, bf16 = jnp.float32, jnp.bfloat16
    proj_rows = model_width // sp_count
    rows_total = sp_count * capacity
    shape = jax.ShapeDtypeStruct
    group = (across, capacity, width)
    return pl.pallas_call(
        functools.partial(fused_kernel, sp_count, tp_count),
        out_shape=(
            shape((tok_count, width), bf16),
            shape((tok_count, channels), bf16),
            shape((tok_count, channels), bf16),
            shape((proj_rows, channels), f32),
            shape((1, model_width, hidden), f32),
            shape((1, model_width, hidden), f32),
            shape((1, hidden, model_width), f32),
        ),
        in_specs=[pl.BlockSpec(memory_space=vmem)] + [pl.BlockSpec(memory_space=pl.ANY)] * 10,
        out_specs=[pl.BlockSpec(memory_space=vmem)] * 4 + [pl.BlockSpec(memory_space=pl.ANY)] * 3,
        scratch_shapes=[
            vmem((2, tok_count, model_width), bf16),
            vmem((model_width, 2 * hidden), bf16),
            vmem((hidden, model_width), bf16),
            vmem(conv_saved.shape, bf16),
            vmem(out_proj.shape, bf16),
            vmem(conv_taps.shape, f32),
            vmem(conv_saved.shape, bf16),
            vmem(conv_saved.shape, bf16),
            vmem((layers, 8, tok_count), f32),
            vmem((2, layers, tok_count, width), bf16),
            vmem((2, sp_count, capacity, model_width), bf16),
            vmem((across, capacity, tok_count), bf16),
            vmem((across, capacity, 128), f32),
            vmem((2, across - 1, chips, capacity, width), bf16),
            vmem((2, layers - 1, across - 1, capacity, width), bf16),
            vmem((tok_count, tok_count), bf16),
            vmem((rows_total, tok_count), bf16),
            vmem((tok_count, rows_total), bf16),
            vmem((hidden, rows_total), bf16),
            vmem((rows_total, 2 * hidden), bf16),
            vmem((sp_count, capacity, model_width), bf16),
            vmem((layers, chips) + group, bf16),
            vmem((layers, chips - 1) + group, bf16),
            vmem((layers, chips - 1) + group, bf16),
            vmem((layers,) + group, bf16),
            vmem((sp_count, capacity, width), bf16),
            vmem((tok_count, model_width), bf16),
            vmem((2, 8, 128), f32),
            vmem((2, tp_count, 8, 128), f32),
            vmem((sp_count, proj_rows, channels), bf16),
            vmem((sp_count, proj_rows, channels), bf16),
            vmem((rim, channels), f32),
            vmem((tok_count + rim, channels), f32),
            vmem((model_width, hidden), f32),
            vmem((model_width, hidden), f32),
            vmem((hidden, model_width), f32),
            dma((10,)),
            dma((3, model_width // 256)),
            dma((layers,)),
            dma((layers,)),
            dma((2, layers, 2)),
            dma((2, layers)),
        ]
        + [dma((2, layers, across - 1, chips))] * 2
        + [dma((2, layers, across, chips - 1))] * 2
        + [dma((2, layers, across, chips))] * 2
        + [dma((layers, chips))] * 2
        + [dma((layers, chips - 1))] * 2
        + [dma((layers, across)), dma((sp_count,))]
        + [dma((2, chips))] * 2
        + [dma((2, tp_count))] * 2
        + [dma((sp_count,))] * 2
        + [dma((1,))] * 2,
        compiler_params=pltpu.CompilerParams(
            collective_id=0, has_side_effects=True, vmem_limit_bytes=60 * 1024 * 1024
        ),
        name="fused",
    )(meta, stream, upstream, gate_w, up_w, down_w, *conv_args)


def on_device(
    upstream,
    stream,
    routes,
    route_weights,
    glu_value,
    glu_gate,
    conv_taps,
    conv_saved,
    out_proj,
    expert_gate,
    expert_up,
    expert_down,
):
    tok_count = upstream.shape[0]
    expert_count = lax.axis_size("sp")
    capacity = 4 * tok_count // expert_count
    meta = jnp.concatenate(
        [
            routes.T.astype(jnp.float32),
            route_weights.T,
            jnp.zeros((8 - 2 * routes.shape[1], tok_count), jnp.float32),
        ]
    )
    return fused(
        expert_count,
        lax.axis_size("tp"),
        capacity,
        meta,
        stream,
        upstream,
        expert_gate,
        expert_up,
        expert_down,
        conv_saved,
        out_proj,
        conv_taps,
        glu_value,
        glu_gate,
    )


def solution(mesh):
    in_specs = (
        P("sp", None),
        P("sp", None),
        P("sp", None),
        P("sp", None),
        P("sp", "tp"),
        P("sp", "tp"),
        P(None, "tp"),
        P("sp", "tp"),
        P(None, "tp"),
        P("sp", None, "tp"),
        P("sp", None, "tp"),
        P("sp", "tp", None),
    )
    out_specs = (
        P("sp", "tp"),
        P("sp", "tp"),
        P("sp", "tp"),
        P("sp", "tp"),
        P("sp", None, "tp"),
        P("sp", None, "tp"),
        P("sp", "tp", None),
    )
    return jax.shard_map(
        on_device, mesh=mesh, in_specs=in_specs, out_specs=out_specs, check_vma=False
    )
```

```python
import functools

import jax
import jax.numpy as jnp
from jax import lax
from jax.experimental import pallas as pl
from jax.experimental.pallas import tpu as pltpu
from jax.sharding import PartitionSpec as P


clamp_limit = 7.0
glu_alpha = 1.702
norm_eps = 1e-05


def contract_rows(left, right):
    return lax.dot_general(
        left, right, (((0,), (0,)), ((), ())), preferred_element_type=jnp.float32
    )


def times_transposed(left, right):
    return lax.dot_general(
        left, right, (((1,), (1,)), ((), ())), preferred_element_type=jnp.float32
    )


def greet(sp_count, tp_count):
    me, lane = lax.axis_index("sp"), lax.axis_index("tp")
    barrier = pltpu.get_barrier_semaphore()
    for step in range(1, sp_count):
        pl.semaphore_signal(
            barrier,
            inc=1,
            device_id={"sp": lax.rem(me + step, sp_count)},
            device_id_type=pl.DeviceIdType.MESH,
        )
    for step in range(1, tp_count):
        pl.semaphore_signal(
            barrier,
            inc=1,
            device_id={"tp": lax.rem(lane + step, tp_count)},
            device_id_type=pl.DeviceIdType.MESH,
        )
    pl.semaphore_wait(barrier, sp_count + tp_count - 2)


def remote(src, dst, send_sem, recv_sem, **target):
    return pltpu.make_async_remote_copy(
        src_ref=src,
        dst_ref=dst,
        send_sem=send_sem,
        recv_sem=recv_sem,
        device_id=target,
        device_id_type=pl.DeviceIdType.MESH,
    )


def load_in(src, dst, sem):
    return pltpu.make_async_copy(src, dst, sem)


def fused_kernel(
    sp_count,
    tp_count,
    routes_ref,
    route_weights_ref,
    stream_hbm,
    upstream_hbm,
    gate_hbm,
    up_hbm,
    down_hbm,
    saved_hbm,
    proj_hbm,
    taps_hbm,
    value_hbm,
    conv_gate_hbm,
    grad_stream_ref,
    grad_value_ref,
    grad_gate_ref,
    grad_proj_ref,
    gate_acc,
    up_acc,
    down_acc,
    tokens,
    weights,
    down_ref,
    saved_ref,
    proj_ref,
    taps_ref,
    value_ref,
    gate_ref,
    meta_ref,
    metas,
    chained,
    extra,
    both,
    chosen,
    gains,
    near_out,
    cross_out,
    before,
    picks_all,
    picks_t,
    act_t,
    slopes,
    partial,
    pair_in,
    side_out,
    side_in,
    total,
    returned,
    full,
    stat_out,
    stat_in,
    parts_out,
    parts_in,
    rim_in,
    padded,
    load_sem,
    meta_send,
    meta_recv,
    chain_send,
    chain_recv,
    extra_send,
    extra_recv,
    cross_send,
    cross_recv,
    along_send,
    along_recv,
    twin_send,
    twin_recv,
    pair_send,
    pair_recv,
    side_send,
    side_recv,
    far_send,
    far_recv,
    full_send,
    full_recv,
    stat_send,
    stat_recv,
    parts_send,
    parts_recv,
    rim_send,
    rim_recv,
):
    me, lane = lax.axis_index("sp"), lax.axis_index("tp")
    chips = tp_count // 2
    across = chips
    layers = sp_count // across
    layer, place = lax.div(me, across), lax.rem(me, across)
    core = lax.rem(lane, 2)
    partner = lane + 1 - 2 * core
    tok_count, model_width = tokens.shape[1:]
    capacity = both.shape[2]
    width = model_width // tp_count
    hidden = down_ref.shape[0]
    group_rows = across * capacity
    channels = saved_ref.shape[1]
    conv_width = channels * tp_count
    groups = tok_count // 128
    f32, bf16 = jnp.float32, jnp.bfloat16

    loads = [
        load_in(stream_hbm, tokens.at[0], load_sem.at[0]),
        load_in(upstream_hbm, tokens.at[1], load_sem.at[1]),
        load_in(saved_hbm, saved_ref, load_sem.at[2]),
        load_in(gate_hbm.at[0], weights.at[:, pl.ds(0, hidden)], load_sem.at[3]),
        load_in(up_hbm.at[0], weights.at[:, pl.ds(hidden, hidden)], load_sem.at[4]),
        load_in(down_hbm.at[0], down_ref, load_sem.at[5]),
        load_in(proj_hbm, proj_ref, load_sem.at[6]),
        load_in(taps_hbm, taps_ref, load_sem.at[7]),
        load_in(value_hbm, value_ref, load_sem.at[8]),
        load_in(conv_gate_hbm, gate_ref, load_sem.at[9]),
    ]
    for load in loads:
        load.start()

    meta_ref[...] = jnp.zeros(meta_ref.shape, f32)
    meta_ref[0:2] = routes_ref[...].astype(f32)
    meta_ref[2:4] = route_weights_ref[...]
    before[...] = jnp.where(
        lax.broadcasted_iota(jnp.int32, before.shape, 0)
        < lax.broadcasted_iota(jnp.int32, before.shape, 1),
        1.0,
        0.0,
    ).astype(bf16)

    greet(sp_count, tp_count)
    started = []

    def begin(copy):
        copy.start()
        started.append(copy)

    def columns(column):
        return pl.ds(pl.multiple_of(column * width, width), width)

    def layer_at(step):
        if step == 0:
            return layer
        inner = jnp.minimum(layer, layers - 1 - layer)
        paired = step <= 2 * inner
        reach = jnp.where(paired, (step + 1) // 2, step - inner)
        below = jnp.where(paired, step % 2 == 1, layer > layers - 1 - layer)
        return jnp.where(below, layer - reach, layer + reach)

    at_layer = [layer_at(step) for step in range(layers)]

    def block_at(step, index):
        return at_layer[step] * across + lax.rem(place + across - index, across)

    def give_meta(step):
        return remote(
            meta_ref,
            metas.at[layer],
            meta_send.at[step],
            meta_recv.at[layer],
            sp=lax.rem(me + step * across, sp_count),
        )

    for step in range(1, layers):
        begin(give_meta(step))

    def own_chain(which, up):
        to = me + across if up else me + sp_count - across
        return remote(
            tokens.at[which, :, columns(lane)],
            chained.at[which, layer],
            chain_send.at[which, 0, int(up)],
            chain_recv.at[which, layer],
            sp=lax.rem(to, sp_count),
        )

    def chain_on(which, step):
        source = at_layer[step]
        to = jnp.where(source < layer, me + across, me + sp_count - across)
        return remote(
            chained.at[which, source],
            chained.at[which, source],
            chain_send.at[which, step, 0],
            chain_recv.at[which, source],
            sp=lax.rem(to, sp_count),
        )

    def goes_on(step):
        source = at_layer[step]
        return jnp.where(source < layer, layer < layers - 1, layer > 0)

    for which in range(2):
        loads[which].wait()

        @pl.when(layer < layers - 1)
        def _():
            own_chain(which, True).start()

        @pl.when(layer > 0)
        def _():
            own_chain(which, False).start()

    last = layers - 1
    far_side = jnp.where(layer > last - layer, 0, 1)
    inside = (layer > 0) & (layer < last)

    def column_at(hop):
        return lax.rem(lane + tp_count - 2 * hop, tp_count)

    def extra_copy(side, which, hop, own):
        to = jnp.where(side == 0, me + across, me + sp_count - across)
        here = extra.at[side, which, hop - 1]
        return remote(
            tokens.at[which, :, columns(column_at(hop))] if own else here,
            here,
            extra_send.at[side, which, hop - 1],
            extra_recv.at[side, which, hop - 1],
            sp=lax.rem(to, sp_count),
        )

    def all_extra():
        return [(which, hop) for which in range(2) for hop in range(1, chips)]

    for side, end in ((0, 0), (1, last)):

        @pl.when(layer == end)
        def _():
            for which, hop in all_extra():
                extra_copy(side, which, hop, True).start()

    def stage_near():
        @pl.when(inside)
        def _():
            for which, hop in all_extra():
                extra_copy(1 - far_side, which, hop, False).wait_recv()
                extra_copy(1 - far_side, which, hop, False).start()

    def stage_far():
        @pl.when(inside)
        def _():
            for which, hop in all_extra():
                extra_copy(far_side, which, hop, False).wait_recv()
                extra_copy(far_side, which, hop, False).start()

    def piece(which, block, column):
        return both.at[which, block, :, columns(column)]

    def cross(which, step, index, hop):
        column = column_at(hop)
        if step in (0, last):
            source = near_out.at[min(step, 1), which, index - 1, hop]
        else:
            source = cross_out.at[which, step - 1, index - 1]
        return remote(
            source,
            piece(which, block_at(step, 0), column),
            cross_send.at[which, step, index - 1, hop],
            cross_recv.at[which, step, index - 1, hop],
            sp=layer * across + lax.rem(place + index, across),
        )

    def along(which, step, index, hop):
        here = piece(which, block_at(step, index), lane)
        return remote(
            here,
            here,
            along_send.at[which, step, index, hop - 1],
            along_recv.at[which, step, index, hop - 1],
            tp=lax.rem(lane + 2 * hop, tp_count),
        )

    def twin(which, step, index, hop):
        here = piece(which, block_at(step, index), column_at(hop))
        return remote(
            here,
            here,
            twin_send.at[which, step, index, hop],
            twin_recv.at[which, step, index, hop],
            tp=partner,
        )

    def choose(meta):
        rows = lax.broadcasted_iota(jnp.int32, (8, tok_count), 0) + place
        rows = jnp.where(rows >= across, rows - across, rows) + layer * across
        names = rows.astype(f32)
        hit = jnp.where((meta[0:1] == names) | (meta[1:2] == names), 1.0, 0.0)
        slots = jnp.dot(hit.astype(bf16), before[...], preferred_element_type=f32)
        slot_rows = lax.broadcasted_iota(jnp.int32, (capacity, tok_count), 0).astype(f32)
        for index in range(across):
            pick = jnp.where(
                (slots[index : index + 1] == slot_rows) & (hit[index : index + 1] > 0.0), 1.0, 0.0
            )
            chosen[index] = pick.astype(bf16)
            gain = jnp.where(meta[0:1] == names[index : index + 1], meta[2:3], meta[3:4])
            row_gain = jnp.sum(pick * gain, axis=1, keepdims=True)
            gains[index] = jnp.broadcast_to(row_gain, (capacity, 128))

    def picked(which, index, source):
        rows = jnp.dot(chosen[index], source, preferred_element_type=f32)
        if which == 1:
            rows = rows * gains[index][:, :1]
        return rows.astype(bf16)

    def stage_forward(step):
        @pl.when(goes_on(step))
        def _():
            for which in range(2):
                chain_on(which, step).wait_recv()
                chain_on(which, step).start()

    def stage_select(step):
        if step == 0:
            choose(meta_ref[...])
            for which in range(2):
                for index in range(1, across):
                    for hop in range(chips):
                        near_out[0, which, index - 1, hop] = picked(
                            which, index, tokens[which, :, columns(column_at(hop))]
                        )
                        begin(cross(which, 0, index, hop))
            for which in range(2):
                for column in range(tp_count):
                    both[which, me, :, column * width : (column + 1) * width] = picked(
                        which, 0, tokens[which, :, column * width : (column + 1) * width]
                    )
            return
        source = at_layer[step]
        remote(
            meta_ref, metas.at[source], meta_send.at[0], meta_recv.at[source], sp=lax.rem(me + across, sp_count)
        ).wait_recv()
        choose(metas[source])
        for which in range(2):

            @pl.when(jnp.logical_not(goes_on(step)))
            def _():
                chain_on(which, step).wait_recv()

            for index in range(1, across):
                rows = picked(which, index, chained[which, source])
                if step == last:
                    near_out[1, which, index - 1, 0] = rows
                else:
                    cross_out[which, step - 1, index - 1] = rows
                begin(cross(which, step, index, 0))
            both[which, block_at(step, 0), :, columns(lane)] = picked(which, 0, chained[which, source])
            if step < last:
                for hop in range(1, chips):
                    begin(along(which, step, 0, hop))
            begin(twin(which, step, 0, 0))

    def stage_extra():
        for which, hop in all_extra():

            @pl.when(jnp.logical_not(inside))
            def _():
                extra_copy(far_side, which, hop, False).wait_recv()

            source = extra[far_side, which, hop - 1]
            for index in range(1, across):
                near_out[1, which, index - 1, hop] = picked(which, index, source)
                begin(cross(which, last, index, hop))
            both[which, block_at(last, 0), :, columns(column_at(hop))] = picked(which, 0, source)
            begin(twin(which, last, 0, hop))

    def stage_cross(step):
        for which in range(2):
            for index in range(1, across):
                for hop in range(chips if step in (0, last) else 1):
                    cross(which, step, index, hop).wait_recv()
                    if step not in (0, last):
                        for side in range(1, chips):
                            begin(along(which, step, index, side))
                    begin(twin(which, step, index, hop))

    def stage_along(step):
        if step in (0, last):
            return
        for which in range(2):
            for index in range(across):
                for hop in range(1, chips):
                    along(which, step, index, hop).wait_recv()
                    begin(twin(which, step, index, hop))

    def group_at(step):
        return pl.ds(at_layer[step] * across, across)

    hidden_tile = min(hidden, 256)

    def stage_expert(step):
        for which in range(2):
            for index in range(across):
                if step or index:
                    for hop in range(chips):
                        twin(which, step, index, hop).wait_recv()
        if step == 0:
            for load in loads[3:6]:
                load.wait()
        first = pl.multiple_of(at_layer[step] * group_rows, group_rows)
        rows_at = pl.ds(first, group_rows)

        @pl.loop(0, hidden // hidden_tile)
        def _(tile):
            units = pl.ds(pl.multiple_of(tile * hidden_tile, hidden_tile), hidden_tile)
            up_units = pl.ds(pl.multiple_of(hidden + tile * hidden_tile, hidden_tile), hidden_tile)
            rows = both[0, group_at(step)].reshape(group_rows, model_width)
            cot = both[1, group_at(step)].reshape(group_rows, model_width)
            gate_pre = jnp.dot(rows, weights[:, units], preferred_element_type=f32)
            up_pre = jnp.dot(rows, weights[:, up_units], preferred_element_type=f32)
            grad_act = times_transposed(cot, down_ref[units, :])
            capped = jnp.minimum(gate_pre, clamp_limit)
            clipped = jnp.clip(up_pre, -clamp_limit, clamp_limit)
            sig = jax.nn.sigmoid(glu_alpha * capped)
            gated = capped * sig
            act_t[units, rows_at] = (gated * (clipped + 1.0)).T.astype(bf16)
            slope = sig + glu_alpha * gated * (1.0 - sig)
            slopes[rows_at, units] = jnp.where(
                gate_pre < clamp_limit, grad_act * (clipped + 1.0) * slope, 0.0
            ).astype(bf16)
            slopes[rows_at, up_units] = jnp.where(
                jnp.abs(up_pre) < clamp_limit, grad_act * gated, 0.0
            ).astype(bf16)

        @pl.loop(0, tp_count)
        def _(tile):
            value = times_transposed(slopes[rows_at, :], weights[columns(tile), :])
            partial[group_at(step), :, columns(tile)] = value.astype(bf16).reshape(
                across, capacity, width
            )

        for hop in list(range(1, chips)) + [0]:
            begin(swapped(step, hop))

    def swapped(step, hop):
        other = lax.rem(lane + 2 * hop, tp_count) + 1 - 2 * core
        return remote(
            partial.at[group_at(step), :, columns(other)],
            pair_in.at[step, hop],
            pair_send.at[step, hop],
            pair_recv.at[step, hop],
            tp=partner,
        )

    def beside(step, hop):
        return remote(
            side_out.at[step, hop - 1],
            side_in.at[step, hop - 1],
            side_send.at[step, hop - 1],
            side_recv.at[step, hop - 1],
            tp=lax.rem(lane + 2 * hop, tp_count),
        )

    def pair_sum(step, hop):
        column = lax.rem(lane + 2 * hop, tp_count)
        return partial[group_at(step), :, columns(column)].astype(f32) + pair_in[step, hop].astype(f32)

    def stage_pair(step):
        for hop in range(1, chips):
            swapped(step, hop).wait_recv()
            side_out[step, hop - 1] = pair_sum(step, hop).astype(bf16)
            begin(beside(step, hop))

    def stage_return(step):
        swapped(step, 0).wait_recv()
        value = pair_sum(step, 0)
        for hop in range(1, chips):
            beside(step, hop).wait_recv()
            value += side_in[step, hop - 1].astype(f32)
        total[step] = value.astype(bf16)
        for index in range(across):
            spot = lax.rem(place + index, across)
            if step == 0 and index == 0:
                returned[me] = total[0, spot]
            else:
                begin(
                    remote(
                        total.at[step, spot],
                        returned.at[me],
                        far_send.at[step, index],
                        far_recv.at[me],
                        sp=at_layer[step] * across + spot,
                    )
                )

    stage_select(0)

    eye = (
        lax.broadcasted_iota(jnp.int32, (128, 128), 0)
        == lax.broadcasted_iota(jnp.int32, (128, 128), 1)
    )

    def stat(phase, hop):
        return remote(
            stat_out.at[phase],
            stat_in.at[phase, hop],
            stat_send.at[phase, hop],
            stat_recv.at[phase, hop],
            tp=lax.rem(lane + hop, tp_count),
        )

    def share(phase, sums):
        stat_out[phase] = jnp.zeros(stat_out.shape[1:], f32)
        row = 0
        for item in sums:
            for group in range(groups):
                part = item[group * 128 : (group + 1) * 128]
                spread = jnp.where(eye, jnp.broadcast_to(part, (128, 128)), 0.0)
                stat_out[phase, row : row + 1] = jnp.sum(spread, axis=0, keepdims=True)
                row += 1
        for hop in range(1, tp_count):
            begin(stat(phase, hop))

    def shared(phase):
        value = stat_out[phase]
        for hop in range(1, tp_count):
            stat(phase, hop).wait_recv()
            value += stat_in[phase, hop]
        columns_of = []
        for item in range(2):
            parts = []
            for group in range(groups):
                row = item * groups + group
                spread = jnp.broadcast_to(value[row : row + 1], (128, 128))
                parts.append(jnp.sum(jnp.where(eye, spread, 0.0), axis=1, keepdims=True))
            columns_of.append(jnp.concatenate(parts, axis=0))
        return columns_of

    loads[2].wait()
    first_conv = saved_ref[...].astype(f32)
    share(
        0,
        (
            jnp.sum(first_conv, axis=1, keepdims=True),
            jnp.sum(first_conv * first_conv, axis=1, keepdims=True),
        ),
    )

    own_meta = meta_ref[...]
    names = lax.broadcasted_iota(jnp.int32, (sp_count, tok_count), 0).astype(f32)
    hit = jnp.where((own_meta[0:1] == names) | (own_meta[1:2] == names), 1.0, 0.0)
    slots = jnp.dot(hit.astype(bf16), before[...], preferred_element_type=f32)
    slot_rows = lax.broadcasted_iota(jnp.int32, (capacity, tok_count), 0).astype(f32)
    for expert in range(sp_count):
        pick = jnp.where(
            (slots[expert : expert + 1] == slot_rows) & (hit[expert : expert + 1] > 0.0), 1.0, 0.0
        )
        picks_all[expert * capacity : (expert + 1) * capacity] = pick.astype(bf16)
    picks_t[...] = picks_all[...].astype(f32).T.astype(bf16)

    stage_forward(1)
    stage_select(1)
    for step in range(2, min(3, layers)):
        stage_forward(step)
    stage_cross(0)
    stage_expert(0)
    stage_pair(0)
    for step in range(2, layers):
        if step == 2:
            stage_cross(1)
        stage_select(step)
        if step == 2:
            stage_near()
        if step + 1 < layers:
            stage_forward(step + 1)
        stage_along(step - 1)
        if step < last:
            stage_cross(step)
        if step == last:
            stage_far()
        stage_expert(step - 1)
        stage_return(step - 2)
        stage_pair(step - 1)
    stage_extra()
    stage_cross(last)
    stage_expert(last)
    stage_return(last - 1)
    stage_pair(last)

    tile_width = 256
    tiles = model_width // tile_width
    rows_total = sp_count * capacity

    @pl.loop(0, tiles)
    def _(tile):
        at = pl.ds(pl.multiple_of(tile * tile_width, tile_width), tile_width)
        down_acc[0, :, at] = jnp.dot(
            act_t[...], both[1, :, :, at].reshape(rows_total, tile_width), preferred_element_type=f32
        )

    stage_return(layers - 1)

    @pl.loop(0, tiles)
    def _(tile):
        at = pl.ds(pl.multiple_of(tile * tile_width, tile_width), tile_width)
        left = both[0, :, :, at].reshape(rows_total, tile_width)
        gate_acc[0, at] = contract_rows(left, slopes[:, :hidden])
        up_acc[0, at] = contract_rows(left, slopes[:, hidden:])

    total_sum, square_sum = shared(0)
    mean_c = total_sum / conv_width
    var_c = square_sum / conv_width - mean_c * mean_c
    inv_std = lax.rsqrt(var_c + norm_eps)
    saved_conv = saved_ref[...].astype(f32)
    normed = (saved_conv - mean_c) * inv_std
    norm_sigmoid = jax.nn.sigmoid(normed)
    mixed = (normed * norm_sigmoid).astype(bf16)
    for load in loads[6:]:
        load.wait()

    for step in range(1, sp_count):
        source = lax.rem(me + step, sp_count)
        remote(
            total.at[0, 0], returned.at[source], far_send.at[0, 0], far_recv.at[source], sp=source
        ).wait_recv()
    routed_sum = jnp.dot(
        picks_t[...],
        returned[...].reshape(-1, width),
        preferred_element_type=f32,
    )
    own_grad = (tokens[1, :, columns(lane)].astype(f32) + routed_sum).astype(bf16)
    grad_stream_ref[...] = own_grad
    full[:, columns(lane)] = own_grad

    def spread_full(hop):
        return remote(
            full.at[:, columns(lane)],
            full.at[:, columns(lane)],
            full_send.at[0, hop],
            full_recv.at[0, hop],
            tp=lax.rem(lane + 2 * hop, tp_count),
        )

    def hand_over(hop):
        column = lax.rem(lane + tp_count - 2 * hop, tp_count)
        return remote(
            full.at[:, columns(column)],
            full.at[:, columns(column)],
            full_send.at[1, hop],
            full_recv.at[1, hop],
            tp=partner,
        )

    for hop in range(1, chips):
        begin(spread_full(hop))
    begin(hand_over(0))
    for hop in range(1, chips):
        spread_full(hop).wait_recv()
        begin(hand_over(hop))
    for hop in range(chips):
        hand_over(hop).wait_recv()

    for column in range(tp_count):
        block = contract_rows(full[:, column * width : (column + 1) * width], mixed)
        per = sp_count // tp_count
        parts_out[column * per : (column + 1) * per] = block.reshape(
            per, width // per, channels
        ).astype(bf16)

    def give_parts(step):
        to = lax.rem(me + step, sp_count)
        return remote(
            parts_out.at[to],
            parts_in.at[step],
            parts_send.at[step],
            parts_recv.at[step],
            sp=to,
        )

    for step in range(1, sp_count):
        begin(give_parts(step))

    grad_mixed = jnp.dot(full[...], proj_ref[...], preferred_element_type=f32)
    grad_normed = grad_mixed * norm_sigmoid * (1.0 + normed * (1.0 - norm_sigmoid))
    share(
        1,
        (
            jnp.sum(grad_normed, axis=1, keepdims=True),
            jnp.sum(grad_normed * normed, axis=1, keepdims=True),
        ),
    )
    first_sum, second_sum = shared(1)
    grad_conv = inv_std * (
        grad_normed - first_sum / conv_width - normed * (second_sum / conv_width)
    )
    padded[:tok_count] = grad_conv
    rim = rim_in.shape[0]
    rim_copy = remote(
        padded.at[pl.ds(0, rim)],
        rim_in,
        rim_send.at[0],
        rim_recv.at[0],
        sp=lax.rem(me + sp_count - 1, sp_count),
    )
    begin(rim_copy)
    gate_sig = jax.nn.sigmoid(gate_ref[...].astype(f32))
    rim_copy.wait_recv()
    padded[tok_count:] = jnp.where(me == sp_count - 1, 0.0, rim_in[...])
    grad_glu = jnp.zeros((tok_count, channels), f32)
    for offset in range(taps_ref.shape[0]):
        grad_glu += taps_ref[offset : offset + 1] * padded[offset : offset + tok_count]
    grad_value_ref[...] = (grad_glu * gate_sig).astype(bf16)
    grad_gate_ref[...] = (
        grad_glu * value_ref[...].astype(f32) * gate_sig * (1.0 - gate_sig)
    ).astype(bf16)

    summed = parts_out[me].astype(f32)
    for step in range(1, sp_count):
        give_parts(step).wait_recv()
        summed += parts_in[step].astype(f32)
    grad_proj_ref[...] = summed
    for copy in started:
        copy.wait_send()
    for side, end in ((0, 0), (1, last)):

        @pl.when(layer == end)
        def _():
            for which, hop in all_extra():
                extra_copy(side, which, hop, True).wait_send()

    @pl.when(inside)
    def _():
        for side in range(2):
            for which, hop in all_extra():
                extra_copy(side, which, hop, False).wait_send()

    for which in range(2):

        @pl.when(layer < layers - 1)
        def _():
            own_chain(which, True).wait_send()

        @pl.when(layer > 0)
        def _():
            own_chain(which, False).wait_send()

        for step in range(1, layers):

            @pl.when(goes_on(step))
            def _():
                chain_on(which, step).wait_send()


def fused(
    sp_count, tp_count, capacity, routes, gains, stream, upstream, gate_w, up_w, down_w, *conv_args
):
    conv_saved, out_proj, conv_taps = conv_args[:3]
    tok_count, model_width = stream.shape
    channels = conv_saved.shape[1]
    hidden = down_w.shape[1]
    width = model_width // tp_count
    chips = tp_count // 2
    across = chips
    layers = sp_count // across
    rim = -(-(conv_taps.shape[0] - 1) // 8) * 8
    dma, vmem = pltpu.SemaphoreType.DMA, pltpu.VMEM
    f32, bf16 = jnp.float32, jnp.bfloat16
    proj_rows = model_width // sp_count
    rows_total = sp_count * capacity
    shape = pltpu.VMEM
    group = (across, capacity, width)
    return pl.pallas_call(
        functools.partial(fused_kernel, sp_count, tp_count),
        out_shape=(
            shape((tok_count, width), bf16),
            shape((tok_count, channels), bf16),
            shape((tok_count, channels), bf16),
            shape((proj_rows, channels), f32),
            shape((1, model_width, hidden), f32),
            shape((1, model_width, hidden), f32),
            shape((1, hidden, model_width), f32),
        ),
        in_specs=[pl.BlockSpec(memory_space=vmem)] * 2 + [pl.BlockSpec(memory_space=pl.ANY)] * 10,
        out_specs=[pl.BlockSpec(memory_space=vmem)] * 7,
        scratch_shapes=[
            vmem((2, tok_count, model_width), bf16),
            vmem((model_width, 2 * hidden), bf16),
            vmem((hidden, model_width), bf16),
            vmem(conv_saved.shape, bf16),
            vmem(out_proj.shape, bf16),
            vmem(conv_taps.shape, f32),
            vmem(conv_saved.shape, bf16),
            vmem(conv_saved.shape, bf16),
            vmem((8, tok_count), f32),
            vmem((layers, 8, tok_count), f32),
            vmem((2, layers, tok_count, width), bf16),
            vmem((2, 2, chips - 1, tok_count, width), bf16),
            vmem((2, sp_count, capacity, model_width), bf16),
            vmem((across, capacity, tok_count), bf16),
            vmem((across, capacity, 128), f32),
            vmem((2, 2, across - 1, chips, capacity, width), bf16),
            vmem((2, layers - 2, across - 1, capacity, width), bf16),
            vmem((tok_count, tok_count), bf16),
            vmem((rows_total, tok_count), bf16),
            vmem((tok_count, rows_total), bf16),
            vmem((hidden, rows_total), bf16),
            vmem((rows_total, 2 * hidden), bf16),
            vmem((sp_count, capacity, model_width), bf16),
            vmem((layers, chips) + group, bf16),
            vmem((layers, chips - 1) + group, bf16),
            vmem((layers, chips - 1) + group, bf16),
            vmem((layers,) + group, bf16),
            vmem((sp_count, capacity, width), bf16),
            vmem((tok_count, model_width), bf16),
            vmem((2, 8, 128), f32),
            vmem((2, tp_count, 8, 128), f32),
            vmem((sp_count, proj_rows, channels), bf16),
            vmem((sp_count, proj_rows, channels), bf16),
            vmem((rim, channels), f32),
            vmem((tok_count + rim, channels), f32),
            dma((10,)),
            dma((layers,)),
            dma((layers,)),
            dma((2, layers, 2)),
            dma((2, layers)),
            dma((2, 2, chips - 1)),
            dma((2, 2, chips - 1)),
        ]
        + [dma((2, layers, across - 1, chips))] * 2
        + [dma((2, layers, across, chips - 1))] * 2
        + [dma((2, layers, across, chips))] * 2
        + [dma((layers, chips))] * 2
        + [dma((layers, chips - 1))] * 2
        + [dma((layers, across)), dma((sp_count,))]
        + [dma((2, chips))] * 2
        + [dma((2, tp_count))] * 2
        + [dma((sp_count,))] * 2
        + [dma((1,))] * 2,
        compiler_params=pltpu.CompilerParams(
            collective_id=0, has_side_effects=True, vmem_limit_bytes=46 * 1024 * 1024
        ),
        name="fused",
    )(routes, gains, stream, upstream, gate_w, up_w, down_w, *conv_args)


def emit_kernel(*refs):
    count = len(refs) // 2
    copies = [
        pltpu.make_async_copy(refs[at], refs[count + at], refs[-1].at[at]) for at in range(count)
    ]
    for copy in reversed(copies):
        copy.start()
    for copy in copies:
        copy.wait()


def emit(results):
    count = len(results)
    return pl.pallas_call(
        emit_kernel,
        out_shape=tuple(jax.ShapeDtypeStruct(item.shape, item.dtype) for item in results),
        in_specs=[pl.BlockSpec(memory_space=pltpu.VMEM)] * count,
        out_specs=[pl.BlockSpec(memory_space=pl.ANY)] * count,
        scratch_shapes=[pltpu.SemaphoreType.DMA((count,))],
        compiler_params=pltpu.CompilerParams(vmem_limit_bytes=1024 * 1024),
        name="emit",
    )(*[pltpu.with_memory_space_constraint(item, pltpu.VMEM) for item in results])


def on_device(
    upstream,
    stream,
    routes,
    route_weights,
    glu_value,
    glu_gate,
    conv_taps,
    conv_saved,
    out_proj,
    expert_gate,
    expert_up,
    expert_down,
):
    tok_count = upstream.shape[0]
    expert_count = lax.axis_size("sp")
    capacity = 4 * tok_count // expert_count
    results = fused(
        expert_count,
        lax.axis_size("tp"),
        capacity,
        routes.T,
        route_weights.T,
        stream,
        upstream,
        expert_gate,
        expert_up,
        expert_down,
        conv_saved,
        out_proj,
        conv_taps,
        glu_value,
        glu_gate,
    )
    return emit(results)


def solution(mesh):
    in_specs = (
        P("sp", None),
        P("sp", None),
        P("sp", None),
        P("sp", None),
        P("sp", "tp"),
        P("sp", "tp"),
        P(None, "tp"),
        P("sp", "tp"),
        P(None, "tp"),
        P("sp", None, "tp"),
        P("sp", None, "tp"),
        P("sp", "tp", None),
    )
    out_specs = (
        P("sp", "tp"),
        P("sp", "tp"),
        P("sp", "tp"),
        P("sp", "tp"),
        P("sp", None, "tp"),
        P("sp", None, "tp"),
        P("sp", "tp", None),
    )
    return jax.shard_map(
        on_device, mesh=mesh, in_specs=in_specs, out_specs=out_specs, check_vma=False
    )
```

```python
import functools

import jax
import jax.numpy as jnp
from jax import lax
from jax.experimental import pallas as pl
from jax.experimental.pallas import tpu as pltpu
from jax.sharding import PartitionSpec as P


clamp_limit = 7.0
glu_alpha = 1.702
norm_eps = 1e-05


def contract_rows(left, right):
    return lax.dot_general(
        left, right, (((0,), (0,)), ((), ())), preferred_element_type=jnp.float32
    )


def times_transposed(left, right):
    return lax.dot_general(
        left, right, (((1,), (1,)), ((), ())), preferred_element_type=jnp.float32
    )


def greet(sp_count, tp_count):
    me, lane = lax.axis_index("sp"), lax.axis_index("tp")
    barrier = pltpu.get_barrier_semaphore()
    for step in range(1, sp_count):
        pl.semaphore_signal(
            barrier,
            inc=1,
            device_id={"sp": lax.rem(me + step, sp_count)},
            device_id_type=pl.DeviceIdType.MESH,
        )
    for step in range(1, tp_count):
        pl.semaphore_signal(
            barrier,
            inc=1,
            device_id={"tp": lax.rem(lane + step, tp_count)},
            device_id_type=pl.DeviceIdType.MESH,
        )
    pl.semaphore_wait(barrier, sp_count + tp_count - 2)


def remote(src, dst, send_sem, recv_sem, **target):
    return pltpu.make_async_remote_copy(
        src_ref=src,
        dst_ref=dst,
        send_sem=send_sem,
        recv_sem=recv_sem,
        device_id=target,
        device_id_type=pl.DeviceIdType.MESH,
    )


def load_in(src, dst, sem):
    return pltpu.make_async_copy(src, dst, sem)


def fused_kernel(
    sp_count,
    tp_count,
    routes_ref,
    route_weights_ref,
    stream_hbm,
    upstream_hbm,
    gate_hbm,
    up_hbm,
    down_hbm,
    saved_hbm,
    proj_hbm,
    taps_hbm,
    value_hbm,
    conv_gate_hbm,
    grad_stream_ref,
    grad_value_ref,
    grad_gate_ref,
    grad_proj_ref,
    gate_acc,
    up_acc,
    down_acc,
    tokens,
    weights,
    down_ref,
    saved_ref,
    proj_ref,
    taps_ref,
    value_ref,
    gate_ref,
    meta_ref,
    metas,
    chained,
    extra,
    both,
    chosen,
    gains,
    near_out,
    cross_out,
    before,
    picks_all,
    picks_t,
    act_t,
    slopes,
    partial,
    pair_in,
    side_out,
    side_in,
    total,
    returned,
    full,
    stat_out,
    stat_in,
    parts_out,
    parts_in,
    rim_in,
    padded,
    load_sem,
    meta_send,
    meta_recv,
    chain_send,
    chain_recv,
    extra_send,
    extra_recv,
    cross_send,
    cross_recv,
    along_send,
    along_recv,
    twin_send,
    twin_recv,
    pair_send,
    pair_recv,
    side_send,
    side_recv,
    far_send,
    far_recv,
    full_send,
    full_recv,
    stat_send,
    stat_recv,
    parts_send,
    parts_recv,
    rim_send,
    rim_recv,
):
    me, lane = lax.axis_index("sp"), lax.axis_index("tp")
    chips = tp_count // 2
    across = chips
    layers = sp_count // across
    layer, place = lax.div(me, across), lax.rem(me, across)
    core = lax.rem(lane, 2)
    partner = lane + 1 - 2 * core
    tok_count, model_width = tokens.shape[1:]
    capacity = both.shape[2]
    width = model_width // tp_count
    hidden = down_ref.shape[0]
    group_rows = across * capacity
    channels = saved_ref.shape[1]
    conv_width = channels * tp_count
    groups = tok_count // 128
    f32, bf16 = jnp.float32, jnp.bfloat16

    loads = [
        load_in(stream_hbm, tokens.at[0], load_sem.at[0]),
        load_in(upstream_hbm, tokens.at[1], load_sem.at[1]),
        load_in(saved_hbm, saved_ref, load_sem.at[2]),
        load_in(gate_hbm.at[0], weights.at[:, pl.ds(0, hidden)], load_sem.at[3]),
        load_in(up_hbm.at[0], weights.at[:, pl.ds(hidden, hidden)], load_sem.at[4]),
        load_in(down_hbm.at[0], down_ref, load_sem.at[5]),
        load_in(proj_hbm, proj_ref, load_sem.at[6]),
        load_in(taps_hbm, taps_ref, load_sem.at[7]),
        load_in(value_hbm, value_ref, load_sem.at[8]),
        load_in(conv_gate_hbm, gate_ref, load_sem.at[9]),
    ]
    for load in loads:
        load.start()

    meta_ref[...] = jnp.zeros(meta_ref.shape, f32)
    meta_ref[0:2] = routes_ref[...].astype(f32)
    meta_ref[2:4] = route_weights_ref[...]
    before[...] = jnp.where(
        lax.broadcasted_iota(jnp.int32, before.shape, 0)
        < lax.broadcasted_iota(jnp.int32, before.shape, 1),
        1.0,
        0.0,
    ).astype(bf16)

    greet(sp_count, tp_count)
    started = []

    def begin(copy):
        copy.start()
        started.append(copy)

    def columns(column):
        return pl.ds(pl.multiple_of(column * width, width), width)

    def layer_at(step):
        if step == 0:
            return layer
        inner = jnp.minimum(layer, layers - 1 - layer)
        paired = step <= 2 * inner
        reach = jnp.where(paired, (step + 1) // 2, step - inner)
        below = jnp.where(paired, step % 2 == 1, layer > layers - 1 - layer)
        return jnp.where(below, layer - reach, layer + reach)

    at_layer = [layer_at(step) for step in range(layers)]

    def block_at(step, index):
        return at_layer[step] * across + lax.rem(place + across - index, across)

    def give_meta(step):
        return remote(
            meta_ref,
            metas.at[layer],
            meta_send.at[step],
            meta_recv.at[layer],
            sp=lax.rem(me + step * across, sp_count),
        )

    for step in range(1, layers):
        begin(give_meta(step))

    def own_chain(which, up):
        to = me + across if up else me + sp_count - across
        return remote(
            tokens.at[which, :, columns(lane)],
            chained.at[which, layer],
            chain_send.at[which, 0, int(up)],
            chain_recv.at[which, layer],
            sp=lax.rem(to, sp_count),
        )

    def chain_on(which, step):
        source = at_layer[step]
        to = jnp.where(source < layer, me + across, me + sp_count - across)
        return remote(
            chained.at[which, source],
            chained.at[which, source],
            chain_send.at[which, step, 0],
            chain_recv.at[which, source],
            sp=lax.rem(to, sp_count),
        )

    def goes_on(step):
        source = at_layer[step]
        return jnp.where(source < layer, layer < layers - 1, layer > 0)

    for which in range(2):
        loads[which].wait()

        @pl.when(layer < layers - 1)
        def _():
            own_chain(which, True).start()

        @pl.when(layer > 0)
        def _():
            own_chain(which, False).start()

    last = layers - 1
    far_side = jnp.where(layer > last - layer, 0, 1)
    inside = (layer > 0) & (layer < last)

    def column_at(hop):
        return lax.rem(lane + tp_count - 2 * hop, tp_count)

    def extra_copy(side, which, hop, own):
        to = jnp.where(side == 0, me + across, me + sp_count - across)
        here = extra.at[side, which, hop - 1]
        return remote(
            tokens.at[which, :, columns(column_at(hop))] if own else here,
            here,
            extra_send.at[side, which, hop - 1],
            extra_recv.at[side, which, hop - 1],
            sp=lax.rem(to, sp_count),
        )

    def all_extra():
        return [(which, hop) for which in range(2) for hop in range(1, chips)]

    for side, end in ((0, 0), (1, last)):

        @pl.when(layer == end)
        def _():
            for which, hop in all_extra():
                extra_copy(side, which, hop, True).start()

    def stage_near():
        @pl.when(inside)
        def _():
            for which, hop in all_extra():
                extra_copy(1 - far_side, which, hop, False).wait_recv()
                extra_copy(1 - far_side, which, hop, False).start()

    def piece(which, block, column):
        return both.at[which, block, :, columns(column)]

    def cross(which, step, index, hop):
        column = column_at(hop)
        if step in (0, last):
            source = near_out.at[min(step, 1), which, index - 1, hop]
        else:
            source = cross_out.at[which, step - 1, index - 1]
        return remote(
            source,
            piece(which, block_at(step, 0), column),
            cross_send.at[which, step, index - 1, hop],
            cross_recv.at[which, step, index - 1, hop],
            sp=layer * across + lax.rem(place + index, across),
        )

    def along(which, step, index, hop):
        here = piece(which, block_at(step, index), lane)
        return remote(
            here,
            here,
            along_send.at[which, step - 1, index, hop - 1],
            along_recv.at[which, step - 1, index, hop - 1],
            tp=lax.rem(lane + 2 * hop, tp_count),
        )

    def twin(which, step, index, hop):
        here = piece(which, block_at(step, index), column_at(hop))
        return remote(
            here,
            here,
            twin_send.at[which, step, index, hop],
            twin_recv.at[which, step, index, hop],
            tp=partner,
        )

    def choose(meta):
        rows = lax.broadcasted_iota(jnp.int32, (8, tok_count), 0) + place
        rows = jnp.where(rows >= across, rows - across, rows) + layer * across
        names = rows.astype(f32)
        hit = jnp.where((meta[0:1] == names) | (meta[1:2] == names), 1.0, 0.0)
        slots = jnp.dot(hit.astype(bf16), before[...], preferred_element_type=f32)
        slot_rows = lax.broadcasted_iota(jnp.int32, (capacity, tok_count), 0).astype(f32)
        for index in range(across):
            pick = jnp.where(
                (slots[index : index + 1] == slot_rows) & (hit[index : index + 1] > 0.0), 1.0, 0.0
            )
            chosen[index] = pick.astype(bf16)
            gain = jnp.where(meta[0:1] == names[index : index + 1], meta[2:3], meta[3:4])
            row_gain = jnp.sum(pick * gain, axis=1, keepdims=True)
            gains[index] = jnp.broadcast_to(row_gain, (capacity, 128))

    def picked(which, index, source):
        rows = jnp.dot(chosen[index], source, preferred_element_type=f32)
        if which == 1:
            rows = rows * gains[index][:, :1]
        return rows.astype(bf16)

    def stage_forward(step):
        @pl.when(goes_on(step))
        def _():
            for which in range(2):
                chain_on(which, step).wait_recv()
                chain_on(which, step).start()

    def stage_select(step):
        if step == 0:
            choose(meta_ref[...])
            for which in range(2):
                for index in range(1, across):
                    for hop in range(chips):
                        near_out[0, which, index - 1, hop] = picked(
                            which, index, tokens[which, :, columns(column_at(hop))]
                        )
                        begin(cross(which, 0, index, hop))
            for which in range(2):
                for column in range(tp_count):
                    both[which, me, :, column * width : (column + 1) * width] = picked(
                        which, 0, tokens[which, :, column * width : (column + 1) * width]
                    )
            return
        source = at_layer[step]
        remote(
            meta_ref, metas.at[source], meta_send.at[0], meta_recv.at[source], sp=lax.rem(me + across, sp_count)
        ).wait_recv()
        choose(metas[source])
        for which in range(2):

            @pl.when(jnp.logical_not(goes_on(step)))
            def _():
                chain_on(which, step).wait_recv()

            for index in range(1, across):
                rows = picked(which, index, chained[which, source])
                cross_out[which, step - 1, index - 1] = rows
                begin(cross(which, step, index, 0))
            both[which, block_at(step, 0), :, columns(lane)] = picked(which, 0, chained[which, source])
            for hop in range(1, chips):
                begin(along(which, step, 0, hop))
            begin(twin(which, step, 0, 0))

    def send_last(which, hop, source):
        for index in range(1, across):
            near_out[1, which, index - 1, hop] = picked(which, index, source)
            cross(which, last, index, hop).start()
        both[which, block_at(last, 0), :, columns(column_at(hop))] = picked(which, 0, source)
        twin(which, last, 0, hop).start()

    def select_last(wait):
        source = at_layer[last]
        remote(
            meta_ref, metas.at[source], meta_send.at[0], meta_recv.at[source], sp=lax.rem(me + across, sp_count)
        ).wait_recv()
        choose(metas[source])
        for which in range(2):
            if wait:
                chain_on(which, last).wait_recv()
            send_last(which, 0, chained[which, source])

    def stage_inner():
        @pl.when(inside)
        def _():
            select_last(False)

    def stage_outer():
        @pl.when(jnp.logical_not(inside))
        def _():
            select_last(True)

    def stage_far():
        @pl.when(inside)
        def _():
            for which, hop in all_extra():
                extra_copy(far_side, which, hop, False).wait_recv()
                extra_copy(far_side, which, hop, False).start()
            for which, hop in all_extra():
                send_last(which, hop, extra[far_side, which, hop - 1])

    def stage_extra():
        @pl.when(jnp.logical_not(inside))
        def _():
            for which, hop in all_extra():
                extra_copy(far_side, which, hop, False).wait_recv()
                send_last(which, hop, extra[far_side, which, hop - 1])

        for which in range(2):
            for hop in range(chips):
                started.append(twin(which, last, 0, hop))
                for index in range(1, across):
                    started.append(cross(which, last, index, hop))

    def stage_cross(step):
        for which in range(2):
            for index in range(1, across):
                for hop in range(chips if step in (0, last) else 1):
                    cross(which, step, index, hop).wait_recv()
                    if step not in (0, last):
                        for side in range(1, chips):
                            begin(along(which, step, index, side))
                    begin(twin(which, step, index, hop))

    def stage_along(step):
        if step in (0, last):
            return
        for which in range(2):
            for index in range(across):
                for hop in range(1, chips):
                    along(which, step, index, hop).wait_recv()
                    begin(twin(which, step, index, hop))

    split_last = capacity % 128 == 0

    def blocks_of(step, index):
        if index is None:
            return at_layer[step] * across, across
        return block_at(step, index), 1

    def group_at(step, index):
        first, count = blocks_of(step, index)
        return pl.ds(first, count)

    def slot_of(step, index):
        return step + (index or 0)

    hidden_tile = min(hidden, 256)

    def stage_expert(step, part=None):
        for which in range(2):
            for index in range(across) if part is None else [part]:
                if step or index:
                    for hop in range(chips):
                        twin(which, step, index, hop).wait_recv()
        if step == 0:
            for load in loads[3:6]:
                load.wait()
        first, count = blocks_of(step, part)
        size = count * capacity
        rows_at = pl.ds(pl.multiple_of(first * capacity, size), size)
        group = group_at(step, part)

        @pl.loop(0, hidden // hidden_tile)
        def _(tile):
            units = pl.ds(pl.multiple_of(tile * hidden_tile, hidden_tile), hidden_tile)
            up_units = pl.ds(pl.multiple_of(hidden + tile * hidden_tile, hidden_tile), hidden_tile)
            rows = both[0, group].reshape(size, model_width)
            cot = both[1, group].reshape(size, model_width)
            gate_pre = jnp.dot(rows, weights[:, units], preferred_element_type=f32)
            up_pre = jnp.dot(rows, weights[:, up_units], preferred_element_type=f32)
            grad_act = times_transposed(cot, down_ref[units, :])
            capped = jnp.minimum(gate_pre, clamp_limit)
            clipped = jnp.clip(up_pre, -clamp_limit, clamp_limit)
            sig = jax.nn.sigmoid(glu_alpha * capped)
            gated = capped * sig
            act_t[units, rows_at] = (gated * (clipped + 1.0)).T.astype(bf16)
            slope = sig + glu_alpha * gated * (1.0 - sig)
            slopes[rows_at, units] = jnp.where(
                gate_pre < clamp_limit, grad_act * (clipped + 1.0) * slope, 0.0
            ).astype(bf16)
            slopes[rows_at, up_units] = jnp.where(
                jnp.abs(up_pre) < clamp_limit, grad_act * gated, 0.0
            ).astype(bf16)

        @pl.loop(0, tp_count)
        def _(tile):
            value = times_transposed(slopes[rows_at, :], weights[columns(tile), :])
            partial[group, :, columns(tile)] = value.astype(bf16).reshape(count, capacity, width)

        for hop in list(range(1, chips)) + [0]:
            begin(swapped(step, hop, part))

    def swapped(step, hop, part):
        other = lax.rem(lane + 2 * hop, tp_count) + 1 - 2 * core
        slot, count = slot_of(step, part), blocks_of(step, part)[1]
        return remote(
            partial.at[group_at(step, part), :, columns(other)],
            pair_in.at[slot, hop, pl.ds(0, count)],
            pair_send.at[slot, hop],
            pair_recv.at[slot, hop],
            tp=partner,
        )

    def beside(step, hop, part):
        slot, count = slot_of(step, part), blocks_of(step, part)[1]
        return remote(
            side_out.at[slot, hop - 1, pl.ds(0, count)],
            side_in.at[slot, hop - 1, pl.ds(0, count)],
            side_send.at[slot, hop - 1],
            side_recv.at[slot, hop - 1],
            tp=lax.rem(lane + 2 * hop, tp_count),
        )

    def pair_sum(step, hop, part):
        column = lax.rem(lane + 2 * hop, tp_count)
        slot, count = slot_of(step, part), blocks_of(step, part)[1]
        mine = partial[group_at(step, part), :, columns(column)].astype(f32)
        return mine + pair_in[slot, hop, pl.ds(0, count)].astype(f32)

    def stage_pair(step, part=None):
        slot, count = slot_of(step, part), blocks_of(step, part)[1]
        for hop in range(1, chips):
            swapped(step, hop, part).wait_recv()
            side_out[slot, hop - 1, pl.ds(0, count)] = pair_sum(step, hop, part).astype(bf16)
            begin(beside(step, hop, part))

    def stage_return(step, part=None):
        slot, count = slot_of(step, part), blocks_of(step, part)[1]
        swapped(step, 0, part).wait_recv()
        value = pair_sum(step, 0, part)
        for hop in range(1, chips):
            beside(step, hop, part).wait_recv()
            value += side_in[slot, hop - 1, pl.ds(0, count)].astype(f32)
        total[slot, pl.ds(0, count)] = value.astype(bf16)
        for index in range(across) if part is None else [part]:
            block = block_at(step, index)
            spot = lax.rem(place + across - index, across) if part is None else 0
            if step == 0 and index == 0:
                returned[me] = total[0, spot]
            else:
                begin(
                    remote(
                        total.at[slot, spot],
                        returned.at[me],
                        far_send.at[step, index],
                        far_recv.at[me],
                        sp=block,
                    )
                )

    stage_select(0)

    eye = (
        lax.broadcasted_iota(jnp.int32, (128, 128), 0)
        == lax.broadcasted_iota(jnp.int32, (128, 128), 1)
    )

    def stat(phase, hop):
        return remote(
            stat_out.at[phase],
            stat_in.at[phase, hop],
            stat_send.at[phase, hop - 1],
            stat_recv.at[phase, hop - 1],
            tp=lax.rem(lane + hop, tp_count),
        )

    def share(phase, sums):
        stat_out[phase] = jnp.zeros(stat_out.shape[1:], f32)
        row = 0
        for item in sums:
            for group in range(groups):
                part = item[group * 128 : (group + 1) * 128]
                spread = jnp.where(eye, jnp.broadcast_to(part, (128, 128)), 0.0)
                stat_out[phase, row : row + 1] = jnp.sum(spread, axis=0, keepdims=True)
                row += 1
        for hop in range(1, tp_count):
            begin(stat(phase, hop))

    def shared(phase):
        value = stat_out[phase]
        for hop in range(1, tp_count):
            stat(phase, hop).wait_recv()
            value += stat_in[phase, hop]
        columns_of = []
        for item in range(2):
            parts = []
            for group in range(groups):
                row = item * groups + group
                spread = jnp.broadcast_to(value[row : row + 1], (128, 128))
                parts.append(jnp.sum(jnp.where(eye, spread, 0.0), axis=1, keepdims=True))
            columns_of.append(jnp.concatenate(parts, axis=0))
        return columns_of

    loads[2].wait()
    first_conv = saved_ref[...].astype(f32)
    share(
        0,
        (
            jnp.sum(first_conv, axis=1, keepdims=True),
            jnp.sum(first_conv * first_conv, axis=1, keepdims=True),
        ),
    )

    own_meta = meta_ref[...]
    names = lax.broadcasted_iota(jnp.int32, (sp_count, tok_count), 0).astype(f32)
    hit = jnp.where((own_meta[0:1] == names) | (own_meta[1:2] == names), 1.0, 0.0)
    slots = jnp.dot(hit.astype(bf16), before[...], preferred_element_type=f32)
    slot_rows = lax.broadcasted_iota(jnp.int32, (capacity, tok_count), 0).astype(f32)
    for expert in range(sp_count):
        pick = jnp.where(
            (slots[expert : expert + 1] == slot_rows) & (hit[expert : expert + 1] > 0.0), 1.0, 0.0
        )
        picks_all[expert * capacity : (expert + 1) * capacity] = pick.astype(bf16)
    picks_t[...] = picks_all[...].astype(f32).T.astype(bf16)

    stage_forward(1)
    stage_select(1)
    for step in range(2, min(3, layers)):
        stage_forward(step)
    stage_cross(0)
    stage_expert(0)
    stage_pair(0)
    for step in range(2, layers):
        if step == 2:
            stage_cross(1)
        if step < last:
            stage_select(step)
        else:
            stage_outer()
        if step == 2:
            stage_near()
        if step + 1 < layers:
            stage_forward(step + 1)
        if step == last - 1:
            stage_inner()
        stage_along(step - 1)
        if step < last:
            stage_cross(step)
        if step == last - 1:
            stage_far()
        if step < last:
            stage_return(step - 2)
        stage_expert(step - 1)
        if step == last:
            stage_extra()
            stage_return(step - 2)
        stage_pair(step - 1)
    if split_last:
        stage_expert(last, 0)
        stage_pair(last, 0)
        stage_cross(last)
        stage_return(last - 1)
        for index in range(1, across):
            stage_expert(last, index)
            stage_return(last, index - 1)
            stage_pair(last, index)
    else:
        stage_cross(last)
        stage_expert(last)
        stage_return(last - 1)
        stage_pair(last)

    tile_width = 256
    tiles = model_width // tile_width
    rows_total = sp_count * capacity

    @pl.loop(0, tiles)
    def _(tile):
        at = pl.ds(pl.multiple_of(tile * tile_width, tile_width), tile_width)
        down_acc[0, :, at] = jnp.dot(
            act_t[...], both[1, :, :, at].reshape(rows_total, tile_width), preferred_element_type=f32
        )

    def gate_up_tile(tile):
        at = pl.ds(pl.multiple_of(tile * tile_width, tile_width), tile_width)
        left = both[0, :, :, at].reshape(rows_total, tile_width)
        gate_acc[0, at] = contract_rows(left, slopes[:, :hidden])
        up_acc[0, at] = contract_rows(left, slopes[:, hidden:])

    pl.loop(0, tiles // 4)(gate_up_tile)
    stage_return(last, across - 1 if split_last else None)
    pl.loop(tiles // 4, tiles)(gate_up_tile)

    total_sum, square_sum = shared(0)
    mean_c = total_sum / conv_width
    var_c = square_sum / conv_width - mean_c * mean_c
    inv_std = lax.rsqrt(var_c + norm_eps)
    saved_conv = saved_ref[...].astype(f32)
    normed = (saved_conv - mean_c) * inv_std
    norm_sigmoid = jax.nn.sigmoid(normed)
    mixed = (normed * norm_sigmoid).astype(bf16)
    for load in loads[6:]:
        load.wait()

    for step in range(1, sp_count):
        source = lax.rem(me + step, sp_count)
        remote(
            total.at[0, 0], returned.at[source], far_send.at[0, 0], far_recv.at[source], sp=source
        ).wait_recv()
    routed_sum = jnp.dot(
        picks_t[...],
        returned[...].reshape(-1, width),
        preferred_element_type=f32,
    )
    own_grad = (tokens[1, :, columns(lane)].astype(f32) + routed_sum).astype(bf16)
    grad_stream_ref[...] = own_grad
    full[:, columns(lane)] = own_grad

    def spread_full(hop):
        return remote(
            full.at[:, columns(lane)],
            full.at[:, columns(lane)],
            full_send.at[0, hop],
            full_recv.at[0, hop],
            tp=lax.rem(lane + 2 * hop, tp_count),
        )

    def hand_over(hop):
        column = lax.rem(lane + tp_count - 2 * hop, tp_count)
        return remote(
            full.at[:, columns(column)],
            full.at[:, columns(column)],
            full_send.at[1, hop],
            full_recv.at[1, hop],
            tp=partner,
        )

    for hop in range(1, chips):
        begin(spread_full(hop))
    begin(hand_over(0))
    for hop in range(1, chips):
        spread_full(hop).wait_recv()
        begin(hand_over(hop))
    for hop in range(chips):
        hand_over(hop).wait_recv()

    for column in range(tp_count):
        block = contract_rows(full[:, column * width : (column + 1) * width], mixed)
        per = sp_count // tp_count
        parts_out[column * per : (column + 1) * per] = block.reshape(
            per, width // per, channels
        ).astype(bf16)

    def give_parts(step):
        to = lax.rem(me + step, sp_count)
        return remote(
            parts_out.at[to],
            parts_in.at[step],
            parts_send.at[step],
            parts_recv.at[step],
            sp=to,
        )

    for step in range(1, sp_count):
        begin(give_parts(step))

    grad_mixed = jnp.dot(full[...], proj_ref[...], preferred_element_type=f32)
    grad_normed = grad_mixed * norm_sigmoid * (1.0 + normed * (1.0 - norm_sigmoid))
    share(
        1,
        (
            jnp.sum(grad_normed, axis=1, keepdims=True),
            jnp.sum(grad_normed * normed, axis=1, keepdims=True),
        ),
    )
    first_sum, second_sum = shared(1)
    grad_conv = inv_std * (
        grad_normed - first_sum / conv_width - normed * (second_sum / conv_width)
    )
    padded[:tok_count] = grad_conv
    rim = rim_in.shape[0]
    rim_copy = remote(
        padded.at[pl.ds(0, rim)],
        rim_in,
        rim_send.at[0],
        rim_recv.at[0],
        sp=lax.rem(me + sp_count - 1, sp_count),
    )
    begin(rim_copy)
    gate_sig = jax.nn.sigmoid(gate_ref[...].astype(f32))
    rim_copy.wait_recv()
    padded[tok_count:] = jnp.where(me == sp_count - 1, 0.0, rim_in[...])
    grad_glu = jnp.zeros((tok_count, channels), f32)
    for offset in range(taps_ref.shape[0]):
        grad_glu += taps_ref[offset : offset + 1] * padded[offset : offset + tok_count]
    grad_value_ref[...] = (grad_glu * gate_sig).astype(bf16)
    grad_gate_ref[...] = (
        grad_glu * value_ref[...].astype(f32) * gate_sig * (1.0 - gate_sig)
    ).astype(bf16)

    summed = parts_out[me].astype(f32)
    for step in range(1, sp_count):
        give_parts(step).wait_recv()
        summed += parts_in[step].astype(f32)
    grad_proj_ref[...] = summed
    for copy in started:
        copy.wait_send()
    for side, end in ((0, 0), (1, last)):

        @pl.when(layer == end)
        def _():
            for which, hop in all_extra():
                extra_copy(side, which, hop, True).wait_send()

    @pl.when(inside)
    def _():
        for side in range(2):
            for which, hop in all_extra():
                extra_copy(side, which, hop, False).wait_send()

    for which in range(2):

        @pl.when(layer < layers - 1)
        def _():
            own_chain(which, True).wait_send()

        @pl.when(layer > 0)
        def _():
            own_chain(which, False).wait_send()

        for step in range(1, layers):

            @pl.when(goes_on(step))
            def _():
                chain_on(which, step).wait_send()


def fused(
    sp_count, tp_count, capacity, routes, gains, stream, upstream, gate_w, up_w, down_w, *conv_args
):
    conv_saved, out_proj, conv_taps = conv_args[:3]
    tok_count, model_width = stream.shape
    channels = conv_saved.shape[1]
    hidden = down_w.shape[1]
    width = model_width // tp_count
    chips = tp_count // 2
    across = chips
    layers = sp_count // across
    slots = layers + across - 1
    rim = -(-(conv_taps.shape[0] - 1) // 8) * 8
    dma, vmem = pltpu.SemaphoreType.DMA, pltpu.VMEM
    f32, bf16 = jnp.float32, jnp.bfloat16
    proj_rows = model_width // sp_count
    rows_total = sp_count * capacity
    shape = pltpu.VMEM
    group = (across, capacity, width)
    return pl.pallas_call(
        functools.partial(fused_kernel, sp_count, tp_count),
        out_shape=(
            shape((tok_count, width), bf16),
            shape((tok_count, channels), bf16),
            shape((tok_count, channels), bf16),
            shape((proj_rows, channels), f32),
            shape((1, model_width, hidden), f32),
            shape((1, model_width, hidden), f32),
            shape((1, hidden, model_width), f32),
        ),
        in_specs=[pl.BlockSpec(memory_space=vmem)] * 2 + [pl.BlockSpec(memory_space=pl.ANY)] * 10,
        out_specs=[pl.BlockSpec(memory_space=vmem)] * 7,
        scratch_shapes=[
            vmem((2, tok_count, model_width), bf16),
            vmem((model_width, 2 * hidden), bf16),
            vmem((hidden, model_width), bf16),
            vmem(conv_saved.shape, bf16),
            vmem(out_proj.shape, bf16),
            vmem(conv_taps.shape, f32),
            vmem(conv_saved.shape, bf16),
            vmem(conv_saved.shape, bf16),
            vmem((8, tok_count), f32),
            vmem((layers, 8, tok_count), f32),
            vmem((2, layers, tok_count, width), bf16),
            vmem((2, 2, chips - 1, tok_count, width), bf16),
            vmem((2, sp_count, capacity, model_width), bf16),
            vmem((across, capacity, tok_count), bf16),
            vmem((across, capacity, 128), f32),
            vmem((2, 2, across - 1, chips, capacity, width), bf16),
            vmem((2, layers - 2, across - 1, capacity, width), bf16),
            vmem((tok_count, tok_count), bf16),
            vmem((rows_total, tok_count), bf16),
            vmem((tok_count, rows_total), bf16),
            vmem((hidden, rows_total), bf16),
            vmem((rows_total, 2 * hidden), bf16),
            vmem((sp_count, capacity, model_width), bf16),
            vmem((slots, chips) + group, bf16),
            vmem((slots, chips - 1) + group, bf16),
            vmem((slots, chips - 1) + group, bf16),
            vmem((slots,) + group, bf16),
            vmem((sp_count, capacity, width), bf16),
            vmem((tok_count, model_width), bf16),
            vmem((2, 8, 128), f32),
            vmem((2, tp_count, 8, 128), f32),
            vmem((sp_count, proj_rows, channels), bf16),
            vmem((sp_count, proj_rows, channels), bf16),
            vmem((rim, channels), f32),
            vmem((tok_count + rim, channels), f32),
            dma((10,)),
            dma((layers,)),
            dma((layers,)),
            dma((2, layers, 2)),
            dma((2, layers)),
            dma((2, 2, chips - 1)),
            dma((2, 2, chips - 1)),
        ]
        + [dma((2, layers, across - 1, chips))] * 2
        + [dma((2, layers - 2, across, chips - 1))] * 2
        + [dma((2, layers, across, chips))] * 2
        + [dma((slots, chips))] * 2
        + [dma((slots, chips - 1))] * 2
        + [dma((layers, across)), dma((sp_count,))]
        + [dma((2, chips))] * 2
        + [dma((2, tp_count - 1))] * 2
        + [dma((sp_count,))] * 2
        + [dma((1,))] * 2,
        compiler_params=pltpu.CompilerParams(
            collective_id=0, has_side_effects=True, vmem_limit_bytes=47 * 1024 * 1024
        ),
        name="fused",
    )(routes, gains, stream, upstream, gate_w, up_w, down_w, *conv_args)


def emit_kernel(*refs):
    count = len(refs) // 2
    copies = [
        pltpu.make_async_copy(refs[at], refs[count + at], refs[-1].at[at]) for at in range(count)
    ]
    for copy in reversed(copies):
        copy.start()
    for copy in copies:
        copy.wait()


def emit(results):
    count = len(results)
    return pl.pallas_call(
        emit_kernel,
        out_shape=tuple(jax.ShapeDtypeStruct(item.shape, item.dtype) for item in results),
        in_specs=[pl.BlockSpec(memory_space=pltpu.VMEM)] * count,
        out_specs=[pl.BlockSpec(memory_space=pl.ANY)] * count,
        scratch_shapes=[pltpu.SemaphoreType.DMA((count,))],
        compiler_params=pltpu.CompilerParams(vmem_limit_bytes=1024 * 1024),
        name="emit",
    )(*[pltpu.with_memory_space_constraint(item, pltpu.VMEM) for item in results])


def on_device(
    upstream,
    stream,
    routes,
    route_weights,
    glu_value,
    glu_gate,
    conv_taps,
    conv_saved,
    out_proj,
    expert_gate,
    expert_up,
    expert_down,
):
    tok_count = upstream.shape[0]
    expert_count = lax.axis_size("sp")
    capacity = 4 * tok_count // expert_count
    results = fused(
        expert_count,
        lax.axis_size("tp"),
        capacity,
        routes.T,
        route_weights.T,
        stream,
        upstream,
        expert_gate,
        expert_up,
        expert_down,
        conv_saved,
        out_proj,
        conv_taps,
        glu_value,
        glu_gate,
    )
    return emit(results)


def solution(mesh):
    in_specs = (
        P("sp", None),
        P("sp", None),
        P("sp", None),
        P("sp", None),
        P("sp", "tp"),
        P("sp", "tp"),
        P(None, "tp"),
        P("sp", "tp"),
        P(None, "tp"),
        P("sp", None, "tp"),
        P("sp", None, "tp"),
        P("sp", "tp", None),
    )
    out_specs = (
        P("sp", "tp"),
        P("sp", "tp"),
        P("sp", "tp"),
        P("sp", "tp"),
        P("sp", None, "tp"),
        P("sp", None, "tp"),
        P("sp", "tp", None),
    )
    return jax.shard_map(
        on_device, mesh=mesh, in_specs=in_specs, out_specs=out_specs, check_vma=False
    )
```

```python
import functools

import jax
import jax.numpy as jnp
from jax import lax
from jax.experimental import pallas as pl
from jax.experimental.pallas import tpu as pltpu
from jax.sharding import PartitionSpec as P


clamp_limit = 7.0
glu_alpha = 1.702
norm_eps = 1e-05


def contract_rows(left, right):
    return lax.dot_general(
        left, right, (((0,), (0,)), ((), ())), preferred_element_type=jnp.float32
    )


def times_transposed(left, right):
    return lax.dot_general(
        left, right, (((1,), (1,)), ((), ())), preferred_element_type=jnp.float32
    )


def greet(sp_count, tp_count):
    me, lane = lax.axis_index("sp"), lax.axis_index("tp")
    barrier = pltpu.get_barrier_semaphore()
    for step in range(1, sp_count):
        pl.semaphore_signal(
            barrier,
            inc=1,
            device_id={"sp": lax.rem(me + step, sp_count)},
            device_id_type=pl.DeviceIdType.MESH,
        )
    for step in range(1, tp_count):
        pl.semaphore_signal(
            barrier,
            inc=1,
            device_id={"tp": lax.rem(lane + step, tp_count)},
            device_id_type=pl.DeviceIdType.MESH,
        )
    pl.semaphore_wait(barrier, sp_count + tp_count - 2)


def remote(src, dst, send_sem, recv_sem, **target):
    return pltpu.make_async_remote_copy(
        src_ref=src,
        dst_ref=dst,
        send_sem=send_sem,
        recv_sem=recv_sem,
        device_id=target,
        device_id_type=pl.DeviceIdType.MESH,
    )


def load_in(src, dst, sem):
    return pltpu.make_async_copy(src, dst, sem)


def fused_kernel(
    sp_count,
    tp_count,
    routes_ref,
    route_weights_ref,
    stream_hbm,
    upstream_hbm,
    gate_hbm,
    up_hbm,
    down_hbm,
    saved_hbm,
    proj_hbm,
    taps_hbm,
    value_hbm,
    conv_gate_hbm,
    grad_stream_ref,
    grad_value_ref,
    grad_gate_ref,
    grad_proj_ref,
    gate_acc,
    up_acc,
    down_acc,
    tokens,
    weights,
    down_ref,
    saved_ref,
    proj_ref,
    taps_ref,
    value_ref,
    gate_ref,
    meta_ref,
    metas,
    chained,
    extra,
    both,
    chosen,
    gains,
    near_out,
    cross_out,
    before,
    picks_all,
    picks_t,
    act_t,
    slopes,
    partial,
    pair_in,
    side_out,
    side_in,
    total,
    returned,
    full,
    stat_out,
    stat_in,
    parts_out,
    parts_in,
    rim_in,
    padded,
    load_sem,
    meta_send,
    meta_recv,
    chain_send,
    chain_recv,
    extra_send,
    extra_recv,
    cross_send,
    cross_recv,
    along_send,
    along_recv,
    twin_send,
    twin_recv,
    pair_send,
    pair_recv,
    side_send,
    side_recv,
    far_send,
    far_recv,
    full_send,
    full_recv,
    stat_send,
    stat_recv,
    parts_send,
    parts_recv,
    rim_send,
    rim_recv,
):
    me, lane = lax.axis_index("sp"), lax.axis_index("tp")
    chips = tp_count // 2
    across = chips
    layers = sp_count // across
    layer, place = lax.div(me, across), lax.rem(me, across)
    core = lax.rem(lane, 2)
    partner = lane + 1 - 2 * core
    tok_count, model_width = tokens.shape[1:]
    capacity = both.shape[2]
    width = model_width // tp_count
    hidden = down_ref.shape[0]
    group_rows = across * capacity
    channels = saved_ref.shape[1]
    conv_width = channels * tp_count
    groups = tok_count // 128
    f32, bf16 = jnp.float32, jnp.bfloat16

    loads = [
        load_in(stream_hbm, tokens.at[0], load_sem.at[0]),
        load_in(upstream_hbm, tokens.at[1], load_sem.at[1]),
        load_in(saved_hbm, saved_ref, load_sem.at[2]),
        load_in(gate_hbm.at[0], weights.at[:, pl.ds(0, hidden)], load_sem.at[3]),
        load_in(up_hbm.at[0], weights.at[:, pl.ds(hidden, hidden)], load_sem.at[4]),
        load_in(down_hbm.at[0], down_ref, load_sem.at[5]),
        load_in(proj_hbm, proj_ref, load_sem.at[6]),
        load_in(taps_hbm, taps_ref, load_sem.at[7]),
        load_in(value_hbm, value_ref, load_sem.at[8]),
        load_in(conv_gate_hbm, gate_ref, load_sem.at[9]),
    ]
    for load in loads:
        load.start()

    meta_ref[...] = jnp.zeros(meta_ref.shape, f32)
    meta_ref[0:2] = routes_ref[...].astype(f32)
    meta_ref[2:4] = route_weights_ref[...]
    before[...] = jnp.where(
        lax.broadcasted_iota(jnp.int32, before.shape, 0)
        < lax.broadcasted_iota(jnp.int32, before.shape, 1),
        1.0,
        0.0,
    ).astype(bf16)

    greet(sp_count, tp_count)
    started = []

    def begin(copy):
        copy.start()
        started.append(copy)

    def columns(column):
        return pl.ds(pl.multiple_of(column * width, width), width)

    def layer_at(step):
        if step == 0:
            return layer
        inner = jnp.minimum(layer, layers - 1 - layer)
        paired = step <= 2 * inner
        reach = jnp.where(paired, (step + 1) // 2, step - inner)
        upper = layer > layers - 1 - layer
        below = jnp.where(paired, jnp.logical_xor(upper, step % 2 == 0), upper)
        return jnp.where(below, layer - reach, layer + reach)

    at_layer = [layer_at(step) for step in range(layers)]

    def block_at(step, index):
        return at_layer[step] * across + lax.rem(place + across - index, across)

    def give_meta(step):
        return remote(
            meta_ref,
            metas.at[layer],
            meta_send.at[step],
            meta_recv.at[layer],
            sp=lax.rem(me + step * across, sp_count),
        )

    for step in range(1, layers):
        begin(give_meta(step))

    def own_chain(which, up):
        to = me + across if up else me + sp_count - across
        return remote(
            tokens.at[which, :, columns(lane)],
            chained.at[which, layer],
            chain_send.at[which, 0, int(up)],
            chain_recv.at[which, layer],
            sp=lax.rem(to, sp_count),
        )

    def chain_on(which, step):
        source = at_layer[step]
        to = jnp.where(source < layer, me + across, me + sp_count - across)
        return remote(
            chained.at[which, source],
            chained.at[which, source],
            chain_send.at[which, step, 0],
            chain_recv.at[which, source],
            sp=lax.rem(to, sp_count),
        )

    def goes_on(step):
        source = at_layer[step]
        return jnp.where(source < layer, layer < layers - 1, layer > 0)

    for which in range(2):
        loads[which].wait()

        @pl.when(layer < layers - 1)
        def _():
            own_chain(which, True).start()

        @pl.when(layer > 0)
        def _():
            own_chain(which, False).start()

    last = layers - 1
    far_side = jnp.where(layer > last - layer, 0, 1)
    inside = (layer > 0) & (layer < last)

    def column_at(hop):
        return lax.rem(lane + tp_count - 2 * hop, tp_count)

    def extra_copy(side, which, hop, own):
        to = jnp.where(side == 0, me + across, me + sp_count - across)
        here = extra.at[side, which, hop - 1]
        return remote(
            tokens.at[which, :, columns(column_at(hop))] if own else here,
            here,
            extra_send.at[side, which, hop - 1],
            extra_recv.at[side, which, hop - 1],
            sp=lax.rem(to, sp_count),
        )

    def all_extra():
        return [(which, hop) for which in range(2) for hop in range(1, chips)]

    for side, end in ((0, 0), (1, last)):

        @pl.when(layer == end)
        def _():
            for which, hop in all_extra():
                extra_copy(side, which, hop, True).start()

    def stage_near():
        @pl.when(inside)
        def _():
            for which, hop in all_extra():
                extra_copy(1 - far_side, which, hop, False).wait_recv()
                extra_copy(1 - far_side, which, hop, False).start()

    def piece(which, block, column):
        return both.at[which, block, :, columns(column)]

    def cross(which, step, index, hop):
        column = column_at(hop)
        if step in (0, last):
            source = near_out.at[min(step, 1), which, index - 1, hop]
        else:
            source = cross_out.at[which, step - 1, index - 1]
        return remote(
            source,
            piece(which, block_at(step, 0), column),
            cross_send.at[0 if step in (0, last) else 1],
            cross_recv.at[which, step, index - 1, hop],
            sp=layer * across + lax.rem(place + index, across),
        )

    def along(which, step, index, hop):
        here = piece(which, block_at(step, index), lane)
        return remote(
            here,
            here,
            along_send.at[0],
            along_recv.at[which, step - 1, index, hop - 1],
            tp=lax.rem(lane + 2 * hop, tp_count),
        )

    def twin(which, step, index, hop):
        here = piece(which, block_at(step, index), column_at(hop))
        return remote(
            here,
            here,
            twin_send.at[0],
            twin_recv.at[which, step, index, hop],
            tp=partner,
        )

    def choose(meta):
        rows = lax.broadcasted_iota(jnp.int32, (8, tok_count), 0) + place
        rows = jnp.where(rows >= across, rows - across, rows) + layer * across
        names = rows.astype(f32)
        hit = jnp.where((meta[0:1] == names) | (meta[1:2] == names), 1.0, 0.0)
        slots = jnp.dot(hit.astype(bf16), before[...], preferred_element_type=f32)
        slot_rows = lax.broadcasted_iota(jnp.int32, (capacity, tok_count), 0).astype(f32)
        for index in range(across):
            pick = jnp.where(
                (slots[index : index + 1] == slot_rows) & (hit[index : index + 1] > 0.0), 1.0, 0.0
            )
            chosen[index] = pick.astype(bf16)
            gain = jnp.where(meta[0:1] == names[index : index + 1], meta[2:3], meta[3:4])
            row_gain = jnp.sum(pick * gain, axis=1, keepdims=True)
            gains[index] = jnp.broadcast_to(row_gain, (capacity, 128))

    def picked(which, index, source):
        rows = jnp.dot(chosen[index], source, preferred_element_type=f32)
        if which == 1:
            rows = rows * gains[index][:, :1]
        return rows.astype(bf16)

    def stage_forward(step):
        @pl.when(goes_on(step))
        def _():
            for which in range(2):
                chain_on(which, step).wait_recv()
                chain_on(which, step).start()

    def stage_select(step):
        if step == 0:
            choose(meta_ref[...])
            for which in range(2):
                for index in range(1, across):
                    for hop in range(chips):
                        near_out[0, which, index - 1, hop] = picked(
                            which, index, tokens[which, :, columns(column_at(hop))]
                        )
                        cross(which, 0, index, hop).start()
            for which in range(2):
                for column in range(tp_count):
                    both[which, me, :, column * width : (column + 1) * width] = picked(
                        which, 0, tokens[which, :, column * width : (column + 1) * width]
                    )
            return
        source = at_layer[step]
        remote(
            meta_ref, metas.at[source], meta_send.at[0], meta_recv.at[source], sp=lax.rem(me + across, sp_count)
        ).wait_recv()
        choose(metas[source])
        for which in range(2):

            @pl.when(jnp.logical_not(goes_on(step)))
            def _():
                chain_on(which, step).wait_recv()

            for index in range(1, across):
                rows = picked(which, index, chained[which, source])
                cross_out[which, step - 1, index - 1] = rows
                cross(which, step, index, 0).start()
            both[which, block_at(step, 0), :, columns(lane)] = picked(which, 0, chained[which, source])
            for hop in range(1, chips):
                along(which, step, 0, hop).start()
            twin(which, step, 0, 0).start()

    def send_last(which, hop, source):
        for index in range(1, across):
            near_out[1, which, index - 1, hop] = picked(which, index, source)
            cross(which, last, index, hop).start()
        both[which, block_at(last, 0), :, columns(column_at(hop))] = picked(which, 0, source)
        twin(which, last, 0, hop).start()

    def select_last(wait):
        source = at_layer[last]
        remote(
            meta_ref, metas.at[source], meta_send.at[0], meta_recv.at[source], sp=lax.rem(me + across, sp_count)
        ).wait_recv()
        choose(metas[source])
        for which in range(2):
            if wait:
                chain_on(which, last).wait_recv()
            send_last(which, 0, chained[which, source])

    def stage_inner():
        @pl.when(inside)
        def _():
            select_last(False)

    def stage_outer():
        @pl.when(jnp.logical_not(inside))
        def _():
            select_last(True)

    def stage_far():
        @pl.when(inside)
        def _():
            for which, hop in all_extra():
                extra_copy(far_side, which, hop, False).wait_recv()
                extra_copy(far_side, which, hop, False).start()
            for which, hop in all_extra():
                send_last(which, hop, extra[far_side, which, hop - 1])

    def stage_extra():
        @pl.when(jnp.logical_not(inside))
        def _():
            for which, hop in all_extra():
                extra_copy(far_side, which, hop, False).wait_recv()
                send_last(which, hop, extra[far_side, which, hop - 1])

    def stage_cross(step):
        for which in range(2):
            for index in range(1, across):
                for hop in range(chips if step in (0, last) else 1):
                    cross(which, step, index, hop).wait_recv()
                    if step not in (0, last):
                        for side in range(1, chips):
                            along(which, step, index, side).start()
                    twin(which, step, index, hop).start()

    def stage_along(step):
        if step in (0, last):
            return
        for which in range(2):
            for index in range(across):
                for hop in range(1, chips):
                    along(which, step, index, hop).wait_recv()
                    twin(which, step, index, hop).start()

    split_last = capacity % 128 == 0

    def blocks_of(step, index):
        if index is None:
            return at_layer[step] * across, across
        return block_at(step, index), 1

    def group_at(step, index):
        first, count = blocks_of(step, index)
        return pl.ds(first, count)

    def slot_of(step, index):
        return step + (index or 0)

    hidden_tile = min(hidden, 256)

    def stage_expert(step, part=None):
        for which in range(2):
            for index in range(across) if part is None else [part]:
                if step or index:
                    for hop in range(chips):
                        twin(which, step, index, hop).wait_recv()
        if step == 0:
            for load in loads[3:6]:
                load.wait()
        first, count = blocks_of(step, part)
        size = count * capacity
        rows_at = pl.ds(pl.multiple_of(first * capacity, size), size)
        group = group_at(step, part)

        @pl.loop(0, hidden // hidden_tile)
        def _(tile):
            units = pl.ds(pl.multiple_of(tile * hidden_tile, hidden_tile), hidden_tile)
            up_units = pl.ds(pl.multiple_of(hidden + tile * hidden_tile, hidden_tile), hidden_tile)
            rows = both[0, group].reshape(size, model_width)
            cot = both[1, group].reshape(size, model_width)
            gate_pre = jnp.dot(rows, weights[:, units], preferred_element_type=f32)
            up_pre = jnp.dot(rows, weights[:, up_units], preferred_element_type=f32)
            grad_act = times_transposed(cot, down_ref[units, :])
            capped = jnp.minimum(gate_pre, clamp_limit)
            clipped = jnp.clip(up_pre, -clamp_limit, clamp_limit)
            sig = jax.nn.sigmoid(glu_alpha * capped)
            gated = capped * sig
            act_t[units, rows_at] = (gated * (clipped + 1.0)).T.astype(bf16)
            slope = sig + glu_alpha * gated * (1.0 - sig)
            slopes[rows_at, units] = jnp.where(
                gate_pre < clamp_limit, grad_act * (clipped + 1.0) * slope, 0.0
            ).astype(bf16)
            slopes[rows_at, up_units] = jnp.where(
                jnp.abs(up_pre) < clamp_limit, grad_act * gated, 0.0
            ).astype(bf16)

        @pl.loop(0, tp_count)
        def _(tile):
            value = times_transposed(slopes[rows_at, :], weights[columns(tile), :])
            partial[group, :, columns(tile)] = value.astype(bf16).reshape(count, capacity, width)

        for hop in list(range(1, chips)) + [0]:
            swapped(step, hop, part).start()

    def swapped(step, hop, part):
        other = lax.rem(lane + 2 * hop, tp_count) + 1 - 2 * core
        slot, count = slot_of(step, part), blocks_of(step, part)[1]
        return remote(
            partial.at[group_at(step, part), :, columns(other)],
            pair_in.at[slot, hop, pl.ds(0, count)],
            pair_send.at[0],
            pair_recv.at[slot, hop],
            tp=partner,
        )

    def beside(step, hop, part):
        slot, count = slot_of(step, part), blocks_of(step, part)[1]
        return remote(
            side_out.at[slot, hop - 1, pl.ds(0, count)],
            side_in.at[slot, hop - 1, pl.ds(0, count)],
            side_send.at[0],
            side_recv.at[slot, hop - 1],
            tp=lax.rem(lane + 2 * hop, tp_count),
        )

    def pair_sum(step, hop, part):
        column = lax.rem(lane + 2 * hop, tp_count)
        slot, count = slot_of(step, part), blocks_of(step, part)[1]
        mine = partial[group_at(step, part), :, columns(column)].astype(f32)
        return mine + pair_in[slot, hop, pl.ds(0, count)].astype(f32)

    def stage_pair(step, part=None):
        slot, count = slot_of(step, part), blocks_of(step, part)[1]
        for hop in range(1, chips):
            swapped(step, hop, part).wait_recv()
            side_out[slot, hop - 1, pl.ds(0, count)] = pair_sum(step, hop, part).astype(bf16)
            beside(step, hop, part).start()

    def stage_return(step, part=None):
        slot, count = slot_of(step, part), blocks_of(step, part)[1]
        swapped(step, 0, part).wait_recv()
        value = pair_sum(step, 0, part)
        for hop in range(1, chips):
            beside(step, hop, part).wait_recv()
            value += side_in[slot, hop - 1, pl.ds(0, count)].astype(f32)
        total[slot, pl.ds(0, count)] = value.astype(bf16)
        for index in range(across) if part is None else [part]:
            block = block_at(step, index)
            spot = lax.rem(place + across - index, across) if part is None else 0
            if step == 0 and index == 0:
                returned[me] = total[0, spot]
            else:
                remote(
                    total.at[slot, spot],
                    returned.at[me],
                    far_send.at[0],
                    far_recv.at[me],
                    sp=block,
                ).start()

    stage_select(0)

    eye = (
        lax.broadcasted_iota(jnp.int32, (128, 128), 0)
        == lax.broadcasted_iota(jnp.int32, (128, 128), 1)
    )

    def stat(phase, hop):
        return remote(
            stat_out.at[phase],
            stat_in.at[phase, hop],
            stat_send.at[phase, hop - 1],
            stat_recv.at[phase, hop - 1],
            tp=lax.rem(lane + hop, tp_count),
        )

    def share(phase, sums):
        stat_out[phase] = jnp.zeros(stat_out.shape[1:], f32)
        row = 0
        for item in sums:
            for group in range(groups):
                part = item[group * 128 : (group + 1) * 128]
                spread = jnp.where(eye, jnp.broadcast_to(part, (128, 128)), 0.0)
                stat_out[phase, row : row + 1] = jnp.sum(spread, axis=0, keepdims=True)
                row += 1
        for hop in range(1, tp_count):
            begin(stat(phase, hop))

    def shared(phase):
        value = stat_out[phase]
        for hop in range(1, tp_count):
            stat(phase, hop).wait_recv()
            value += stat_in[phase, hop]
        columns_of = []
        for item in range(2):
            parts = []
            for group in range(groups):
                row = item * groups + group
                spread = jnp.broadcast_to(value[row : row + 1], (128, 128))
                parts.append(jnp.sum(jnp.where(eye, spread, 0.0), axis=1, keepdims=True))
            columns_of.append(jnp.concatenate(parts, axis=0))
        return columns_of

    loads[2].wait()
    first_conv = saved_ref[...].astype(f32)
    share(
        0,
        (
            jnp.sum(first_conv, axis=1, keepdims=True),
            jnp.sum(first_conv * first_conv, axis=1, keepdims=True),
        ),
    )

    own_meta = meta_ref[...]
    names = lax.broadcasted_iota(jnp.int32, (sp_count, tok_count), 0).astype(f32)
    hit = jnp.where((own_meta[0:1] == names) | (own_meta[1:2] == names), 1.0, 0.0)
    slots = jnp.dot(hit.astype(bf16), before[...], preferred_element_type=f32)
    slot_rows = lax.broadcasted_iota(jnp.int32, (capacity, tok_count), 0).astype(f32)
    for expert in range(sp_count):
        pick = jnp.where(
            (slots[expert : expert + 1] == slot_rows) & (hit[expert : expert + 1] > 0.0), 1.0, 0.0
        )
        picks_all[expert * capacity : (expert + 1) * capacity] = pick.astype(bf16)
    picks_t[...] = picks_all[...].astype(f32).T.astype(bf16)

    stage_forward(1)
    stage_select(1)
    for step in range(2, min(3, layers)):
        stage_forward(step)
    stage_cross(0)
    stage_expert(0)
    stage_pair(0)
    for step in range(2, layers):
        if step == 2:
            stage_cross(1)
        if step < last:
            stage_select(step)
        else:
            stage_outer()
        if step == 2:
            stage_near()
        if step + 1 < layers:
            stage_forward(step + 1)
        if step == last - 1:
            stage_inner()
        stage_along(step - 1)
        if step < last:
            stage_cross(step)
        if step == last - 1:
            stage_far()
        if step < last:
            stage_return(step - 2)
        stage_expert(step - 1)
        if step == last:
            stage_extra()
            stage_return(step - 2)
        stage_pair(step - 1)
    if split_last:
        stage_expert(last, 0)
        stage_pair(last, 0)
        stage_cross(last)
        stage_return(last - 1)
        for index in range(1, across):
            stage_expert(last, index)
            stage_return(last, index - 1)
            stage_pair(last, index)
    else:
        stage_cross(last)
        stage_expert(last)
        stage_return(last - 1)
        stage_pair(last)

    tile_width = 256
    tiles = model_width // tile_width
    rows_total = sp_count * capacity

    @pl.loop(0, tiles)
    def _(tile):
        at = pl.ds(pl.multiple_of(tile * tile_width, tile_width), tile_width)
        down_acc[0, :, at] = jnp.dot(
            act_t[...], both[1, :, :, at].reshape(rows_total, tile_width), preferred_element_type=f32
        )

    def gate_up_tile(tile):
        at = pl.ds(pl.multiple_of(tile * tile_width, tile_width), tile_width)
        left = both[0, :, :, at].reshape(rows_total, tile_width)
        gate_acc[0, at] = contract_rows(left, slopes[:, :hidden])
        up_acc[0, at] = contract_rows(left, slopes[:, hidden:])

    pl.loop(0, tiles // 4)(gate_up_tile)
    stage_return(last, across - 1 if split_last else None)
    pl.loop(tiles // 4, tiles)(gate_up_tile)

    total_sum, square_sum = shared(0)
    mean_c = total_sum / conv_width
    var_c = square_sum / conv_width - mean_c * mean_c
    inv_std = lax.rsqrt(var_c + norm_eps)
    saved_conv = saved_ref[...].astype(f32)
    normed = (saved_conv - mean_c) * inv_std
    norm_sigmoid = jax.nn.sigmoid(normed)
    mixed = (normed * norm_sigmoid).astype(bf16)
    for load in loads[6:]:
        load.wait()

    for step in range(1, sp_count):
        source = lax.rem(me + step, sp_count)
        remote(
            total.at[0, 0], returned.at[source], far_send.at[0], far_recv.at[source], sp=source
        ).wait_recv()
    routed_sum = jnp.dot(
        picks_t[...],
        returned[...].reshape(-1, width),
        preferred_element_type=f32,
    )
    own_grad = (tokens[1, :, columns(lane)].astype(f32) + routed_sum).astype(bf16)
    grad_stream_ref[...] = own_grad
    full[:, columns(lane)] = own_grad

    def spread_full(hop):
        return remote(
            full.at[:, columns(lane)],
            full.at[:, columns(lane)],
            full_send.at[0, hop],
            full_recv.at[0, hop],
            tp=lax.rem(lane + 2 * hop, tp_count),
        )

    def hand_over(hop):
        column = lax.rem(lane + tp_count - 2 * hop, tp_count)
        return remote(
            full.at[:, columns(column)],
            full.at[:, columns(column)],
            full_send.at[1, hop],
            full_recv.at[1, hop],
            tp=partner,
        )

    for hop in range(1, chips):
        begin(spread_full(hop))
    begin(hand_over(0))
    for hop in range(1, chips):
        spread_full(hop).wait_recv()
        begin(hand_over(hop))
    for hop in range(chips):
        hand_over(hop).wait_recv()

    for column in range(tp_count):
        block = contract_rows(full[:, column * width : (column + 1) * width], mixed)
        per = sp_count // tp_count
        parts_out[column * per : (column + 1) * per] = block.reshape(
            per, width // per, channels
        ).astype(bf16)

    def give_parts(step):
        to = lax.rem(me + step, sp_count)
        return remote(
            parts_out.at[to],
            parts_in.at[step],
            parts_send.at[step],
            parts_recv.at[step],
            sp=to,
        )

    for step in range(1, sp_count):
        begin(give_parts(step))

    grad_mixed = jnp.dot(full[...], proj_ref[...], preferred_element_type=f32)
    grad_normed = grad_mixed * norm_sigmoid * (1.0 + normed * (1.0 - norm_sigmoid))
    share(
        1,
        (
            jnp.sum(grad_normed, axis=1, keepdims=True),
            jnp.sum(grad_normed * normed, axis=1, keepdims=True),
        ),
    )
    first_sum, second_sum = shared(1)
    grad_conv = inv_std * (
        grad_normed - first_sum / conv_width - normed * (second_sum / conv_width)
    )
    padded[:tok_count] = grad_conv
    rim = rim_in.shape[0]
    rim_copy = remote(
        padded.at[pl.ds(0, rim)],
        rim_in,
        rim_send.at[0],
        rim_recv.at[0],
        sp=lax.rem(me + sp_count - 1, sp_count),
    )
    begin(rim_copy)
    gate_sig = jax.nn.sigmoid(gate_ref[...].astype(f32))
    rim_copy.wait_recv()
    padded[tok_count:] = jnp.where(me == sp_count - 1, 0.0, rim_in[...])
    grad_glu = jnp.zeros((tok_count, channels), f32)
    for offset in range(taps_ref.shape[0]):
        grad_glu += taps_ref[offset : offset + 1] * padded[offset : offset + tok_count]
    grad_value_ref[...] = (grad_glu * gate_sig).astype(bf16)
    grad_gate_ref[...] = (
        grad_glu * value_ref[...].astype(f32) * gate_sig * (1.0 - gate_sig)
    ).astype(bf16)

    summed = parts_out[me].astype(f32)
    for step in range(1, sp_count):
        give_parts(step).wait_recv()
        summed += parts_in[step].astype(f32)
    grad_proj_ref[...] = summed
    for copy in started:
        copy.wait_send()
    for side, end in ((0, 0), (1, last)):

        @pl.when(layer == end)
        def _():
            for which, hop in all_extra():
                extra_copy(side, which, hop, True).wait_send()

    @pl.when(inside)
    def _():
        for side in range(2):
            for which, hop in all_extra():
                extra_copy(side, which, hop, False).wait_send()

    for which in range(2):

        @pl.when(layer < layers - 1)
        def _():
            own_chain(which, True).wait_send()

        @pl.when(layer > 0)
        def _():
            own_chain(which, False).wait_send()

        for step in range(1, layers):

            @pl.when(goes_on(step))
            def _():
                chain_on(which, step).wait_send()

    def drain(ref, sem):
        remote(ref, ref, sem, parts_recv.at[0], tp=partner).wait_send()

    drain(both.at[0, pl.ds(0, sp_count - 1)], twin_send.at[0])
    drain(near_out, cross_send.at[0])
    drain(cross_out, cross_send.at[1])
    drain(both.at[0, pl.ds(0, (layers - 2) * (chips - 1))], along_send.at[0])
    drain(both.at[0, pl.ds(0, sp_count // 2)], pair_send.at[0])
    drain(both.at[0, pl.ds(0, sp_count * (chips - 1) // tp_count)], side_send.at[0])
    drain(returned.at[pl.ds(0, sp_count - 1)], far_send.at[0])


def fused(
    sp_count, tp_count, capacity, routes, gains, stream, upstream, gate_w, up_w, down_w, *conv_args
):
    conv_saved, out_proj, conv_taps = conv_args[:3]
    tok_count, model_width = stream.shape
    channels = conv_saved.shape[1]
    hidden = down_w.shape[1]
    width = model_width // tp_count
    chips = tp_count // 2
    across = chips
    layers = sp_count // across
    slots = layers + across - 1
    rim = -(-(conv_taps.shape[0] - 1) // 8) * 8
    dma, vmem = pltpu.SemaphoreType.DMA, pltpu.VMEM
    f32, bf16 = jnp.float32, jnp.bfloat16
    proj_rows = model_width // sp_count
    rows_total = sp_count * capacity
    shape = pltpu.VMEM
    group = (across, capacity, width)
    return pl.pallas_call(
        functools.partial(fused_kernel, sp_count, tp_count),
        out_shape=(
            shape((tok_count, width), bf16),
            shape((tok_count, channels), bf16),
            shape((tok_count, channels), bf16),
            shape((proj_rows, channels), f32),
            shape((1, model_width, hidden), f32),
            shape((1, model_width, hidden), f32),
            shape((1, hidden, model_width), f32),
        ),
        in_specs=[pl.BlockSpec(memory_space=vmem)] * 2 + [pl.BlockSpec(memory_space=pl.ANY)] * 10,
        out_specs=[pl.BlockSpec(memory_space=vmem)] * 7,
        scratch_shapes=[
            vmem((2, tok_count, model_width), bf16),
            vmem((model_width, 2 * hidden), bf16),
            vmem((hidden, model_width), bf16),
            vmem(conv_saved.shape, bf16),
            vmem(out_proj.shape, bf16),
            vmem(conv_taps.shape, f32),
            vmem(conv_saved.shape, bf16),
            vmem(conv_saved.shape, bf16),
            vmem((8, tok_count), f32),
            vmem((layers, 8, tok_count), f32),
            vmem((2, layers, tok_count, width), bf16),
            vmem((2, 2, chips - 1, tok_count, width), bf16),
            vmem((2, sp_count, capacity, model_width), bf16),
            vmem((across, capacity, tok_count), bf16),
            vmem((across, capacity, 128), f32),
            vmem((2, 2, across - 1, chips, capacity, width), bf16),
            vmem((2, layers - 2, across - 1, capacity, width), bf16),
            vmem((tok_count, tok_count), bf16),
            vmem((rows_total, tok_count), bf16),
            vmem((tok_count, rows_total), bf16),
            vmem((hidden, rows_total), bf16),
            vmem((rows_total, 2 * hidden), bf16),
            vmem((sp_count, capacity, model_width), bf16),
            vmem((slots, chips) + group, bf16),
            vmem((slots, chips - 1) + group, bf16),
            vmem((slots, chips - 1) + group, bf16),
            vmem((slots,) + group, bf16),
            vmem((sp_count, capacity, width), bf16),
            vmem((tok_count, model_width), bf16),
            vmem((2, 8, 128), f32),
            vmem((2, tp_count, 8, 128), f32),
            vmem((sp_count, proj_rows, channels), bf16),
            vmem((sp_count, proj_rows, channels), bf16),
            vmem((rim, channels), f32),
            vmem((tok_count + rim, channels), f32),
            dma((10,)),
            dma((layers,)),
            dma((layers,)),
            dma((2, layers, 2)),
            dma((2, layers)),
            dma((2, 2, chips - 1)),
            dma((2, 2, chips - 1)),
        ]
        + [dma((2,)), dma((2, layers, across - 1, chips))]
        + [dma((1,)), dma((2, layers - 2, across, chips - 1))]
        + [dma((1,)), dma((2, layers, across, chips))]
        + [dma((1,)), dma((slots, chips))]
        + [dma((1,)), dma((slots, chips - 1))]
        + [dma((1,)), dma((sp_count,))]
        + [dma((2, chips))] * 2
        + [dma((2, tp_count - 1))] * 2
        + [dma((sp_count,))] * 2
        + [dma((1,))] * 2,
        compiler_params=pltpu.CompilerParams(
            collective_id=0, has_side_effects=True, vmem_limit_bytes=47 * 1024 * 1024
        ),
        name="fused",
    )(routes, gains, stream, upstream, gate_w, up_w, down_w, *conv_args)


def emit_kernel(*refs):
    count = len(refs) // 2
    copies = [
        pltpu.make_async_copy(refs[at], refs[count + at], refs[-1].at[at]) for at in range(count)
    ]
    for copy in reversed(copies):
        copy.start()
    for copy in copies:
        copy.wait()


def emit(results):
    count = len(results)
    return pl.pallas_call(
        emit_kernel,
        out_shape=tuple(jax.ShapeDtypeStruct(item.shape, item.dtype) for item in results),
        in_specs=[pl.BlockSpec(memory_space=pltpu.VMEM)] * count,
        out_specs=[pl.BlockSpec(memory_space=pl.ANY)] * count,
        scratch_shapes=[pltpu.SemaphoreType.DMA((count,))],
        compiler_params=pltpu.CompilerParams(vmem_limit_bytes=1024 * 1024),
        name="emit",
    )(*[pltpu.with_memory_space_constraint(item, pltpu.VMEM) for item in results])


def on_device(
    upstream,
    stream,
    routes,
    route_weights,
    glu_value,
    glu_gate,
    conv_taps,
    conv_saved,
    out_proj,
    expert_gate,
    expert_up,
    expert_down,
):
    tok_count = upstream.shape[0]
    expert_count = lax.axis_size("sp")
    capacity = 4 * tok_count // expert_count
    results = fused(
        expert_count,
        lax.axis_size("tp"),
        capacity,
        routes.T,
        route_weights.T,
        stream,
        upstream,
        expert_gate,
        expert_up,
        expert_down,
        conv_saved,
        out_proj,
        conv_taps,
        glu_value,
        glu_gate,
    )
    return emit(results)


def solution(mesh):
    in_specs = (
        P("sp", None),
        P("sp", None),
        P("sp", None),
        P("sp", None),
        P("sp", "tp"),
        P("sp", "tp"),
        P(None, "tp"),
        P("sp", "tp"),
        P(None, "tp"),
        P("sp", None, "tp"),
        P("sp", None, "tp"),
        P("sp", "tp", None),
    )
    out_specs = (
        P("sp", "tp"),
        P("sp", "tp"),
        P("sp", "tp"),
        P("sp", "tp"),
        P("sp", None, "tp"),
        P("sp", None, "tp"),
        P("sp", "tp", None),
    )
    return jax.shard_map(
        on_device, mesh=mesh, in_specs=in_specs, out_specs=out_specs, check_vma=False
    )
```

```python
import functools

import jax
import jax.numpy as jnp
from jax import lax
from jax.experimental import pallas as pl
from jax.experimental.pallas import tpu as pltpu
from jax.sharding import PartitionSpec as P


clamp_limit = 7.0
glu_alpha = 1.702
norm_eps = 1e-05


def contract_rows(left, right):
    return lax.dot_general(
        left, right, (((0,), (0,)), ((), ())), preferred_element_type=jnp.float32
    )


def times_transposed(left, right):
    return lax.dot_general(
        left, right, (((1,), (1,)), ((), ())), preferred_element_type=jnp.float32
    )


def greet(sp_count, tp_count):
    me, lane = lax.axis_index("sp"), lax.axis_index("tp")
    barrier = pltpu.get_barrier_semaphore()
    for step in range(1, sp_count):
        pl.semaphore_signal(
            barrier,
            inc=1,
            device_id={"sp": lax.rem(me + step, sp_count)},
            device_id_type=pl.DeviceIdType.MESH,
        )
    for step in range(1, tp_count):
        pl.semaphore_signal(
            barrier,
            inc=1,
            device_id={"tp": lax.rem(lane + step, tp_count)},
            device_id_type=pl.DeviceIdType.MESH,
        )
    pl.semaphore_wait(barrier, sp_count + tp_count - 2)


def remote(src, dst, send_sem, recv_sem, **target):
    return pltpu.make_async_remote_copy(
        src_ref=src,
        dst_ref=dst,
        send_sem=send_sem,
        recv_sem=recv_sem,
        device_id=target,
        device_id_type=pl.DeviceIdType.MESH,
    )


def load_in(src, dst, sem):
    return pltpu.make_async_copy(src, dst, sem)


def fused_kernel(
    sp_count,
    tp_count,
    routes_ref,
    route_weights_ref,
    stream_hbm,
    upstream_hbm,
    gate_hbm,
    up_hbm,
    down_hbm,
    saved_hbm,
    proj_hbm,
    taps_hbm,
    value_hbm,
    conv_gate_hbm,
    grad_stream_ref,
    grad_value_ref,
    grad_gate_ref,
    grad_proj_ref,
    gate_acc,
    up_acc,
    down_acc,
    tokens,
    weights,
    down_ref,
    saved_ref,
    proj_ref,
    taps_ref,
    value_ref,
    gate_ref,
    meta_ref,
    metas,
    chained,
    extra,
    both,
    chosen,
    gains,
    near_out,
    cross_out,
    before,
    picks_all,
    picks_t,
    act_t,
    slopes,
    partial,
    pair_in,
    side_out,
    side_in,
    total,
    returned,
    full,
    stat_out,
    stat_in,
    parts_out,
    parts_in,
    rim_in,
    padded,
    load_sem,
    meta_send,
    meta_recv,
    chain_send,
    chain_recv,
    extra_send,
    extra_recv,
    cross_send,
    cross_recv,
    along_send,
    along_recv,
    twin_send,
    twin_recv,
    pair_send,
    pair_recv,
    side_send,
    side_recv,
    far_send,
    far_recv,
    full_send,
    full_recv,
    stat_send,
    stat_recv,
    parts_send,
    parts_recv,
    rim_send,
    rim_recv,
):
    me, lane = lax.axis_index("sp"), lax.axis_index("tp")
    chips = tp_count // 2
    across = chips
    layers = sp_count // across
    layer, place = lax.div(me, across), lax.rem(me, across)
    core = lax.rem(lane, 2)
    partner = lane + 1 - 2 * core
    tok_count, model_width = tokens.shape[1:]
    capacity = both.shape[2]
    width = model_width // tp_count
    hidden = down_ref.shape[0]
    group_rows = across * capacity
    channels = saved_ref.shape[1]
    conv_width = channels * tp_count
    groups = tok_count // 128
    f32, bf16 = jnp.float32, jnp.bfloat16

    loads = [
        load_in(stream_hbm, tokens.at[0], load_sem.at[0]),
        load_in(upstream_hbm, tokens.at[1], load_sem.at[1]),
        load_in(saved_hbm, saved_ref, load_sem.at[2]),
        load_in(gate_hbm.at[0], weights.at[:, pl.ds(0, hidden)], load_sem.at[3]),
        load_in(up_hbm.at[0], weights.at[:, pl.ds(hidden, hidden)], load_sem.at[4]),
        load_in(down_hbm.at[0], down_ref, load_sem.at[5]),
        load_in(proj_hbm, proj_ref, load_sem.at[6]),
        load_in(taps_hbm, taps_ref, load_sem.at[7]),
        load_in(value_hbm, value_ref, load_sem.at[8]),
        load_in(conv_gate_hbm, gate_ref, load_sem.at[9]),
    ]
    for load in loads:
        load.start()

    meta_ref[...] = jnp.zeros(meta_ref.shape, f32)
    meta_ref[0:2] = routes_ref[...].astype(f32)
    meta_ref[2:4] = route_weights_ref[...]
    before[...] = jnp.where(
        lax.broadcasted_iota(jnp.int32, before.shape, 0)
        < lax.broadcasted_iota(jnp.int32, before.shape, 1),
        1.0,
        0.0,
    ).astype(bf16)

    greet(sp_count, tp_count)
    started = []

    def begin(copy):
        copy.start()
        started.append(copy)

    def columns(column):
        return pl.ds(pl.multiple_of(column * width, width), width)

    def layer_at(step):
        if step == 0:
            return layer
        inner = jnp.minimum(layer, layers - 1 - layer)
        paired = step <= 2 * inner
        reach = jnp.where(paired, (step + 1) // 2, step - inner)
        upper = layer > layers - 1 - layer
        below = jnp.where(paired, jnp.logical_xor(upper, step % 2 == 0), upper)
        return jnp.where(below, layer - reach, layer + reach)

    at_layer = [layer_at(step) for step in range(layers)]

    def block_at(step, index):
        return at_layer[step] * across + lax.rem(place + across - index, across)

    def give_meta(step):
        return remote(
            meta_ref,
            metas.at[layer],
            meta_send.at[0],
            meta_recv.at[layer],
            sp=lax.rem(me + step * across, sp_count),
        )

    for step in range(1, layers):
        give_meta(step).start()

    def own_chain(which, up):
        to = me + across if up else me + sp_count - across
        return remote(
            tokens.at[which, :, columns(lane)],
            chained.at[which, layer],
            chain_send.at[which, 0, int(up)],
            chain_recv.at[which, layer],
            sp=lax.rem(to, sp_count),
        )

    def chain_on(which, step):
        source = at_layer[step]
        to = jnp.where(source < layer, me + across, me + sp_count - across)
        return remote(
            chained.at[which, source],
            chained.at[which, source],
            chain_send.at[which, step, 0],
            chain_recv.at[which, source],
            sp=lax.rem(to, sp_count),
        )

    def goes_on(step):
        source = at_layer[step]
        return jnp.where(source < layer, layer < layers - 1, layer > 0)

    for which in range(2):
        loads[which].wait()

        @pl.when(layer < layers - 1)
        def _():
            own_chain(which, True).start()

        @pl.when(layer > 0)
        def _():
            own_chain(which, False).start()

    last = layers - 1
    far_side = jnp.where(layer > last - layer, 0, 1)
    inside = (layer > 0) & (layer < last)

    def column_at(hop):
        return lax.rem(lane + tp_count - 2 * hop, tp_count)

    def extra_copy(side, which, hop, own):
        to = jnp.where(side == 0, me + across, me + sp_count - across)
        here = extra.at[side, which, hop - 1]
        return remote(
            tokens.at[which, :, columns(column_at(hop))] if own else here,
            here,
            extra_send.at[side, which, hop - 1],
            extra_recv.at[side, which, hop - 1],
            sp=lax.rem(to, sp_count),
        )

    def all_extra():
        return [(which, hop) for which in range(2) for hop in range(1, chips)]

    for side, end in ((0, 0), (1, last)):

        @pl.when(layer == end)
        def _():
            for which, hop in all_extra():
                extra_copy(side, which, hop, True).start()

    def stage_near():
        @pl.when(inside)
        def _():
            for which, hop in all_extra():
                extra_copy(1 - far_side, which, hop, False).wait_recv()
                extra_copy(1 - far_side, which, hop, False).start()

    def piece(which, block, column):
        return both.at[which, block, :, columns(column)]

    def cross(which, step, index, hop):
        column = column_at(hop)
        if step in (0, last):
            source = near_out.at[min(step, 1), which, index - 1, hop]
        else:
            source = cross_out.at[which, step - 1, index - 1]
        return remote(
            source,
            piece(which, block_at(step, 0), column),
            cross_send.at[0 if step in (0, last) else 1],
            cross_recv.at[which, step, index - 1, hop],
            sp=layer * across + lax.rem(place + index, across),
        )

    def along(which, step, index, hop):
        here = piece(which, block_at(step, index), lane)
        return remote(
            here,
            here,
            along_send.at[0],
            along_recv.at[which, step - 1, index, hop - 1],
            tp=lax.rem(lane + 2 * hop, tp_count),
        )

    def twin(which, step, index, hop):
        here = piece(which, block_at(step, index), column_at(hop))
        return remote(
            here,
            here,
            twin_send.at[0],
            twin_recv.at[which, step, index, hop],
            tp=partner,
        )

    def choose(meta):
        rows = lax.broadcasted_iota(jnp.int32, (8, tok_count), 0) + place
        rows = jnp.where(rows >= across, rows - across, rows) + layer * across
        names = rows.astype(f32)
        hit = jnp.where((meta[0:1] == names) | (meta[1:2] == names), 1.0, 0.0)
        slots = jnp.dot(hit.astype(bf16), before[...], preferred_element_type=f32)
        slot_rows = lax.broadcasted_iota(jnp.int32, (capacity, tok_count), 0).astype(f32)
        for index in range(across):
            pick = jnp.where(
                (slots[index : index + 1] == slot_rows) & (hit[index : index + 1] > 0.0), 1.0, 0.0
            )
            chosen[index] = pick.astype(bf16)
            gain = jnp.where(meta[0:1] == names[index : index + 1], meta[2:3], meta[3:4])
            row_gain = jnp.sum(pick * gain, axis=1, keepdims=True)
            gains[index] = jnp.broadcast_to(row_gain, (capacity, 128))

    def picked(which, index, source):
        rows = jnp.dot(chosen[index], source, preferred_element_type=f32)
        if which == 1:
            rows = rows * gains[index][:, :1]
        return rows.astype(bf16)

    def stage_forward(step):
        @pl.when(goes_on(step))
        def _():
            for which in range(2):
                chain_on(which, step).wait_recv()
                chain_on(which, step).start()

    def stage_select(step):
        if step == 0:
            choose(meta_ref[...])
            for which in range(2):
                for index in range(1, across):
                    for hop in range(chips):
                        near_out[0, which, index - 1, hop] = picked(
                            which, index, tokens[which, :, columns(column_at(hop))]
                        )
                        cross(which, 0, index, hop).start()
            for which in range(2):
                for column in range(tp_count):
                    both[which, me, :, column * width : (column + 1) * width] = picked(
                        which, 0, tokens[which, :, column * width : (column + 1) * width]
                    )
            return
        source = at_layer[step]
        remote(
            meta_ref, metas.at[source], meta_send.at[0], meta_recv.at[source], sp=lax.rem(me + across, sp_count)
        ).wait_recv()
        choose(metas[source])
        for which in range(2):

            @pl.when(jnp.logical_not(goes_on(step)))
            def _():
                chain_on(which, step).wait_recv()

            for index in range(1, across):
                rows = picked(which, index, chained[which, source])
                cross_out[which, step - 1, index - 1] = rows
                cross(which, step, index, 0).start()
            both[which, block_at(step, 0), :, columns(lane)] = picked(which, 0, chained[which, source])
            for hop in range(1, chips):
                along(which, step, 0, hop).start()
            twin(which, step, 0, 0).start()

    def send_last(which, hop, source):
        for index in range(1, across):
            near_out[1, which, index - 1, hop] = picked(which, index, source)
            cross(which, last, index, hop).start()
        both[which, block_at(last, 0), :, columns(column_at(hop))] = picked(which, 0, source)
        twin(which, last, 0, hop).start()

    def select_last(wait):
        source = at_layer[last]
        remote(
            meta_ref, metas.at[source], meta_send.at[0], meta_recv.at[source], sp=lax.rem(me + across, sp_count)
        ).wait_recv()
        choose(metas[source])
        for which in range(2):
            if wait:
                chain_on(which, last).wait_recv()
            send_last(which, 0, chained[which, source])

    def stage_inner():
        @pl.when(inside)
        def _():
            select_last(False)

    def stage_outer():
        @pl.when(jnp.logical_not(inside))
        def _():
            select_last(True)

    def stage_far():
        @pl.when(inside)
        def _():
            for which, hop in all_extra():
                extra_copy(far_side, which, hop, False).wait_recv()
                extra_copy(far_side, which, hop, False).start()
            for which, hop in all_extra():
                send_last(which, hop, extra[far_side, which, hop - 1])

    def stage_extra():
        @pl.when(jnp.logical_not(inside))
        def _():
            for which, hop in all_extra():
                extra_copy(far_side, which, hop, False).wait_recv()
                send_last(which, hop, extra[far_side, which, hop - 1])

    def stage_cross(step):
        for which in range(2):
            for index in range(1, across):
                for hop in range(chips if step in (0, last) else 1):
                    cross(which, step, index, hop).wait_recv()
                    if step not in (0, last):
                        for side in range(1, chips):
                            along(which, step, index, side).start()
                    twin(which, step, index, hop).start()

    def stage_along(step):
        if step in (0, last):
            return
        for which in range(2):
            for index in range(across):
                for hop in range(1, chips):
                    along(which, step, index, hop).wait_recv()
                    twin(which, step, index, hop).start()

    split_last = capacity % 128 == 0

    def blocks_of(step, index):
        if index is None:
            return at_layer[step] * across, across
        return block_at(step, index), 1

    def group_at(step, index):
        first, count = blocks_of(step, index)
        return pl.ds(first, count)

    def slot_of(step, index):
        return step + (index or 0)

    hidden_tile = min(hidden, 256)

    def stage_expert(step, part=None):
        for which in range(2):
            for index in range(across) if part is None else [part]:
                if step or index:
                    for hop in range(chips):
                        twin(which, step, index, hop).wait_recv()
        if step == 0:
            for load in loads[3:6]:
                load.wait()
        first, count = blocks_of(step, part)
        size = count * capacity
        rows_at = pl.ds(pl.multiple_of(first * capacity, size), size)
        group = group_at(step, part)

        @pl.loop(0, hidden // hidden_tile)
        def _(tile):
            units = pl.ds(pl.multiple_of(tile * hidden_tile, hidden_tile), hidden_tile)
            up_units = pl.ds(pl.multiple_of(hidden + tile * hidden_tile, hidden_tile), hidden_tile)
            rows = both[0, group].reshape(size, model_width)
            cot = both[1, group].reshape(size, model_width)
            gate_pre = jnp.dot(rows, weights[:, units], preferred_element_type=f32)
            up_pre = jnp.dot(rows, weights[:, up_units], preferred_element_type=f32)
            grad_act = times_transposed(cot, down_ref[units, :])
            capped = jnp.minimum(gate_pre, clamp_limit)
            clipped = jnp.clip(up_pre, -clamp_limit, clamp_limit)
            sig = jax.nn.sigmoid(glu_alpha * capped)
            gated = capped * sig
            act_t[units, rows_at] = (gated * (clipped + 1.0)).T.astype(bf16)
            slope = sig + glu_alpha * gated * (1.0 - sig)
            slopes[rows_at, units] = jnp.where(
                gate_pre < clamp_limit, grad_act * (clipped + 1.0) * slope, 0.0
            ).astype(bf16)
            slopes[rows_at, up_units] = jnp.where(
                jnp.abs(up_pre) < clamp_limit, grad_act * gated, 0.0
            ).astype(bf16)

        @pl.loop(0, tp_count)
        def _(tile):
            value = times_transposed(slopes[rows_at, :], weights[columns(tile), :])
            partial[group, :, columns(tile)] = value.astype(bf16).reshape(count, capacity, width)

        for hop in list(range(1, chips)) + [0]:
            swapped(step, hop, part).start()

    def swapped(step, hop, part):
        other = lax.rem(lane + 2 * hop, tp_count) + 1 - 2 * core
        slot, count = slot_of(step, part), blocks_of(step, part)[1]
        return remote(
            partial.at[group_at(step, part), :, columns(other)],
            pair_in.at[slot, hop, pl.ds(0, count)],
            pair_send.at[0],
            pair_recv.at[slot, hop],
            tp=partner,
        )

    def beside(step, hop, part):
        slot, count = slot_of(step, part), blocks_of(step, part)[1]
        return remote(
            side_out.at[slot, hop - 1, pl.ds(0, count)],
            side_in.at[slot, hop - 1, pl.ds(0, count)],
            side_send.at[0],
            side_recv.at[slot, hop - 1],
            tp=lax.rem(lane + 2 * hop, tp_count),
        )

    def pair_sum(step, hop, part):
        column = lax.rem(lane + 2 * hop, tp_count)
        slot, count = slot_of(step, part), blocks_of(step, part)[1]
        mine = partial[group_at(step, part), :, columns(column)].astype(f32)
        return mine + pair_in[slot, hop, pl.ds(0, count)].astype(f32)

    def stage_pair(step, part=None):
        slot, count = slot_of(step, part), blocks_of(step, part)[1]
        for hop in range(1, chips):
            swapped(step, hop, part).wait_recv()
            side_out[slot, hop - 1, pl.ds(0, count)] = pair_sum(step, hop, part).astype(bf16)
            beside(step, hop, part).start()

    def stage_return(step, part=None):
        slot, count = slot_of(step, part), blocks_of(step, part)[1]
        swapped(step, 0, part).wait_recv()
        value = pair_sum(step, 0, part)
        for hop in range(1, chips):
            beside(step, hop, part).wait_recv()
            value += side_in[slot, hop - 1, pl.ds(0, count)].astype(f32)
        total[slot, pl.ds(0, count)] = value.astype(bf16)
        for index in range(across) if part is None else [part]:
            block = block_at(step, index)
            spot = lax.rem(place + across - index, across) if part is None else 0
            if step == 0 and index == 0:
                returned[me] = total[0, spot]
            else:
                remote(
                    total.at[slot, spot],
                    returned.at[me],
                    far_send.at[0],
                    far_recv.at[me],
                    sp=block,
                ).start()

    stage_select(0)

    eye = (
        lax.broadcasted_iota(jnp.int32, (128, 128), 0)
        == lax.broadcasted_iota(jnp.int32, (128, 128), 1)
    )

    def stat(phase, hop):
        return remote(
            stat_out.at[phase],
            stat_in.at[phase, hop],
            stat_send.at[0],
            stat_recv.at[phase, hop - 1],
            tp=lax.rem(lane + hop, tp_count),
        )

    def share(phase, sums):
        stat_out[phase] = jnp.zeros(stat_out.shape[1:], f32)
        row = 0
        for item in sums:
            for group in range(groups):
                part = item[group * 128 : (group + 1) * 128]
                spread = jnp.where(eye, jnp.broadcast_to(part, (128, 128)), 0.0)
                stat_out[phase, row : row + 1] = jnp.sum(spread, axis=0, keepdims=True)
                row += 1
        for hop in range(1, tp_count):
            stat(phase, hop).start()

    def shared(phase):
        value = stat_out[phase]
        for hop in range(1, tp_count):
            stat(phase, hop).wait_recv()
            value += stat_in[phase, hop]
        columns_of = []
        for item in range(2):
            parts = []
            for group in range(groups):
                row = item * groups + group
                spread = jnp.broadcast_to(value[row : row + 1], (128, 128))
                parts.append(jnp.sum(jnp.where(eye, spread, 0.0), axis=1, keepdims=True))
            columns_of.append(jnp.concatenate(parts, axis=0))
        return columns_of

    loads[2].wait()
    first_conv = saved_ref[...].astype(f32)
    share(
        0,
        (
            jnp.sum(first_conv, axis=1, keepdims=True),
            jnp.sum(first_conv * first_conv, axis=1, keepdims=True),
        ),
    )

    own_meta = meta_ref[...]
    names = lax.broadcasted_iota(jnp.int32, (sp_count, tok_count), 0).astype(f32)
    hit = jnp.where((own_meta[0:1] == names) | (own_meta[1:2] == names), 1.0, 0.0)
    slots = jnp.dot(hit.astype(bf16), before[...], preferred_element_type=f32)
    slot_rows = lax.broadcasted_iota(jnp.int32, (capacity, tok_count), 0).astype(f32)
    for expert in range(sp_count):
        pick = jnp.where(
            (slots[expert : expert + 1] == slot_rows) & (hit[expert : expert + 1] > 0.0), 1.0, 0.0
        )
        picks_all[expert * capacity : (expert + 1) * capacity] = pick.astype(bf16)
    picks_t[...] = picks_all[...].astype(f32).T.astype(bf16)

    stage_forward(1)
    stage_select(1)
    for step in range(2, min(3, layers)):
        stage_forward(step)
    stage_cross(0)
    stage_expert(0)
    if layers > 2:
        stage_cross(1)
    stage_pair(0)
    for step in range(2, layers):
        if step < last:
            stage_select(step)
        else:
            stage_outer()
        if step == 2:
            stage_near()
        if step + 1 < layers:
            stage_forward(step + 1)
        if step == last - 1:
            stage_inner()
        stage_along(step - 1)
        if step < last:
            stage_cross(step)
        if step == last - 1:
            stage_far()
        if step < last:
            stage_return(step - 2)
        stage_expert(step - 1)
        if step == last:
            stage_extra()
        stage_pair(step - 1)
        if step == last:
            stage_return(step - 2)
    if split_last:
        stage_expert(last, 0)
        stage_pair(last, 0)
        stage_cross(last)
        stage_return(last - 1)
        for index in range(1, across):
            stage_expert(last, index)
            stage_return(last, index - 1)
            stage_pair(last, index)
    else:
        stage_cross(last)
        stage_expert(last)
        stage_return(last - 1)
        stage_pair(last)

    tile_width = 256
    tiles = model_width // tile_width
    rows_total = sp_count * capacity

    @pl.loop(0, tiles)
    def _(tile):
        at = pl.ds(pl.multiple_of(tile * tile_width, tile_width), tile_width)
        down_acc[0, :, at] = jnp.dot(
            act_t[...], both[1, :, :, at].reshape(rows_total, tile_width), preferred_element_type=f32
        )

    def gate_up_tile(tile):
        at = pl.ds(pl.multiple_of(tile * tile_width, tile_width), tile_width)
        left = both[0, :, :, at].reshape(rows_total, tile_width)
        gate_acc[0, at] = contract_rows(left, slopes[:, :hidden])
        up_acc[0, at] = contract_rows(left, slopes[:, hidden:])

    pl.loop(0, tiles // 4)(gate_up_tile)
    stage_return(last, across - 1 if split_last else None)
    pl.loop(tiles // 4, tiles)(gate_up_tile)

    total_sum, square_sum = shared(0)
    mean_c = total_sum / conv_width
    var_c = square_sum / conv_width - mean_c * mean_c
    inv_std = lax.rsqrt(var_c + norm_eps)
    saved_conv = saved_ref[...].astype(f32)
    normed = (saved_conv - mean_c) * inv_std
    norm_sigmoid = jax.nn.sigmoid(normed)
    mixed = (normed * norm_sigmoid).astype(bf16)
    for load in loads[6:]:
        load.wait()

    for step in range(1, sp_count):
        source = lax.rem(me + step, sp_count)
        remote(
            total.at[0, 0], returned.at[source], far_send.at[0], far_recv.at[source], sp=source
        ).wait_recv()
    routed_sum = jnp.dot(
        picks_t[...],
        returned[...].reshape(-1, width),
        preferred_element_type=f32,
    )
    own_grad = (tokens[1, :, columns(lane)].astype(f32) + routed_sum).astype(bf16)
    grad_stream_ref[...] = own_grad
    full[:, columns(lane)] = own_grad

    def spread_full(hop):
        return remote(
            full.at[:, columns(lane)],
            full.at[:, columns(lane)],
            full_send.at[0],
            full_recv.at[0, hop],
            tp=lax.rem(lane + 2 * hop, tp_count),
        )

    def hand_over(hop):
        column = lax.rem(lane + tp_count - 2 * hop, tp_count)
        return remote(
            full.at[:, columns(column)],
            full.at[:, columns(column)],
            full_send.at[0],
            full_recv.at[1, hop],
            tp=partner,
        )

    for hop in range(1, chips):
        spread_full(hop).start()
    hand_over(0).start()
    for hop in range(1, chips):
        spread_full(hop).wait_recv()
        hand_over(hop).start()
    for hop in range(chips):
        hand_over(hop).wait_recv()

    for column in range(tp_count):
        block = contract_rows(full[:, column * width : (column + 1) * width], mixed)
        per = sp_count // tp_count
        parts_out[column * per : (column + 1) * per] = block.reshape(
            per, width // per, channels
        ).astype(bf16)

    def give_parts(step):
        to = lax.rem(me + step, sp_count)
        return remote(
            parts_out.at[to],
            parts_in.at[step],
            parts_send.at[0],
            parts_recv.at[step],
            sp=to,
        )

    for step in range(1, sp_count):
        give_parts(step).start()

    grad_mixed = jnp.dot(full[...], proj_ref[...], preferred_element_type=f32)
    grad_normed = grad_mixed * norm_sigmoid * (1.0 + normed * (1.0 - norm_sigmoid))
    share(
        1,
        (
            jnp.sum(grad_normed, axis=1, keepdims=True),
            jnp.sum(grad_normed * normed, axis=1, keepdims=True),
        ),
    )
    first_sum, second_sum = shared(1)
    grad_conv = inv_std * (
        grad_normed - first_sum / conv_width - normed * (second_sum / conv_width)
    )
    padded[:tok_count] = grad_conv
    rim = rim_in.shape[0]
    rim_copy = remote(
        padded.at[pl.ds(0, rim)],
        rim_in,
        rim_send.at[0],
        rim_recv.at[0],
        sp=lax.rem(me + sp_count - 1, sp_count),
    )
    begin(rim_copy)
    gate_sig = jax.nn.sigmoid(gate_ref[...].astype(f32))
    rim_copy.wait_recv()
    padded[tok_count:] = jnp.where(me == sp_count - 1, 0.0, rim_in[...])
    grad_glu = jnp.zeros((tok_count, channels), f32)
    for offset in range(taps_ref.shape[0]):
        grad_glu += taps_ref[offset : offset + 1] * padded[offset : offset + tok_count]
    grad_value_ref[...] = (grad_glu * gate_sig).astype(bf16)
    grad_gate_ref[...] = (
        grad_glu * value_ref[...].astype(f32) * gate_sig * (1.0 - gate_sig)
    ).astype(bf16)

    summed = parts_out[me].astype(f32)
    for step in range(1, sp_count):
        give_parts(step).wait_recv()
        summed += parts_in[step].astype(f32)
    grad_proj_ref[...] = summed
    for copy in started:
        copy.wait_send()
    for side, end in ((0, 0), (1, last)):

        @pl.when(layer == end)
        def _():
            for which, hop in all_extra():
                extra_copy(side, which, hop, True).wait_send()

    @pl.when(inside)
    def _():
        for side in range(2):
            for which, hop in all_extra():
                extra_copy(side, which, hop, False).wait_send()

    for which in range(2):

        @pl.when(layer < layers - 1)
        def _():
            own_chain(which, True).wait_send()

        @pl.when(layer > 0)
        def _():
            own_chain(which, False).wait_send()

        for step in range(1, layers):

            @pl.when(goes_on(step))
            def _():
                chain_on(which, step).wait_send()

    def drain(ref, sem):
        remote(ref, ref, sem, parts_recv.at[0], tp=partner).wait_send()

    drain(both.at[0, pl.ds(0, sp_count - 1)], twin_send.at[0])
    drain(near_out, cross_send.at[0])
    drain(cross_out, cross_send.at[1])
    drain(both.at[0, pl.ds(0, (layers - 2) * (chips - 1))], along_send.at[0])
    drain(both.at[0, pl.ds(0, sp_count // 2)], pair_send.at[0])
    drain(both.at[0, pl.ds(0, sp_count * (chips - 1) // tp_count)], side_send.at[0])
    drain(returned.at[pl.ds(0, sp_count - 1)], far_send.at[0])
    drain(parts_in.at[pl.ds(0, sp_count - 1)], parts_send.at[0])
    drain(full.at[:, pl.ds(0, (tp_count - 1) * width)], full_send.at[0])
    drain(stat_in.at[:, pl.ds(0, tp_count - 1)], stat_send.at[0])
    drain(metas.at[pl.ds(0, layers - 1)], meta_send.at[0])


def fused(
    sp_count, tp_count, capacity, routes, gains, stream, upstream, gate_w, up_w, down_w, *conv_args
):
    conv_saved, out_proj, conv_taps = conv_args[:3]
    tok_count, model_width = stream.shape
    channels = conv_saved.shape[1]
    hidden = down_w.shape[1]
    width = model_width // tp_count
    chips = tp_count // 2
    across = chips
    layers = sp_count // across
    slots = layers + across - 1
    rim = -(-(conv_taps.shape[0] - 1) // 8) * 8
    dma, vmem = pltpu.SemaphoreType.DMA, pltpu.VMEM
    f32, bf16 = jnp.float32, jnp.bfloat16
    proj_rows = model_width // sp_count
    rows_total = sp_count * capacity
    shape = pltpu.VMEM
    group = (across, capacity, width)
    return pl.pallas_call(
        functools.partial(fused_kernel, sp_count, tp_count),
        out_shape=(
            shape((tok_count, width), bf16),
            shape((tok_count, channels), bf16),
            shape((tok_count, channels), bf16),
            shape((proj_rows, channels), f32),
            shape((1, model_width, hidden), f32),
            shape((1, model_width, hidden), f32),
            shape((1, hidden, model_width), f32),
        ),
        in_specs=[pl.BlockSpec(memory_space=vmem)] * 2 + [pl.BlockSpec(memory_space=pl.ANY)] * 10,
        out_specs=[pl.BlockSpec(memory_space=vmem)] * 7,
        scratch_shapes=[
            vmem((2, tok_count, model_width), bf16),
            vmem((model_width, 2 * hidden), bf16),
            vmem((hidden, model_width), bf16),
            vmem(conv_saved.shape, bf16),
            vmem(out_proj.shape, bf16),
            vmem(conv_taps.shape, f32),
            vmem(conv_saved.shape, bf16),
            vmem(conv_saved.shape, bf16),
            vmem((8, tok_count), f32),
            vmem((layers, 8, tok_count), f32),
            vmem((2, layers, tok_count, width), bf16),
            vmem((2, 2, chips - 1, tok_count, width), bf16),
            vmem((2, sp_count, capacity, model_width), bf16),
            vmem((across, capacity, tok_count), bf16),
            vmem((across, capacity, 128), f32),
            vmem((2, 2, across - 1, chips, capacity, width), bf16),
            vmem((2, layers - 2, across - 1, capacity, width), bf16),
            vmem((tok_count, tok_count), bf16),
            vmem((rows_total, tok_count), bf16),
            vmem((tok_count, rows_total), bf16),
            vmem((hidden, rows_total), bf16),
            vmem((rows_total, 2 * hidden), bf16),
            vmem((sp_count, capacity, model_width), bf16),
            vmem((slots, chips) + group, bf16),
            vmem((slots, chips - 1) + group, bf16),
            vmem((slots, chips - 1) + group, bf16),
            vmem((slots,) + group, bf16),
            vmem((sp_count, capacity, width), bf16),
            vmem((tok_count, model_width), bf16),
            vmem((2, 8, 128), f32),
            vmem((2, tp_count, 8, 128), f32),
            vmem((sp_count, proj_rows, channels), bf16),
            vmem((sp_count, proj_rows, channels), bf16),
            vmem((rim, channels), f32),
            vmem((tok_count + rim, channels), f32),
            dma((10,)),
            dma((1,)),
            dma((layers,)),
            dma((2, layers, 2)),
            dma((2, layers)),
            dma((2, 2, chips - 1)),
            dma((2, 2, chips - 1)),
        ]
        + [dma((2,)), dma((2, layers, across - 1, chips))]
        + [dma((1,)), dma((2, layers - 2, across, chips - 1))]
        + [dma((1,)), dma((2, layers, across, chips))]
        + [dma((1,)), dma((slots, chips))]
        + [dma((1,)), dma((slots, chips - 1))]
        + [dma((1,)), dma((sp_count,))]
        + [dma((1,)), dma((2, chips))]
        + [dma((1,)), dma((2, tp_count - 1))]
        + [dma((1,)), dma((sp_count,))]
        + [dma((1,))] * 2,
        compiler_params=pltpu.CompilerParams(
            collective_id=0, has_side_effects=True, vmem_limit_bytes=47 * 1024 * 1024
        ),
        name="fused",
    )(routes, gains, stream, upstream, gate_w, up_w, down_w, *conv_args)


def emit_kernel(*refs):
    count = len(refs) // 2
    copies = [
        pltpu.make_async_copy(refs[at], refs[count + at], refs[-1].at[at]) for at in range(count)
    ]
    for copy in reversed(copies):
        copy.start()
    for copy in copies:
        copy.wait()


def emit(results):
    count = len(results)
    return pl.pallas_call(
        emit_kernel,
        out_shape=tuple(jax.ShapeDtypeStruct(item.shape, item.dtype) for item in results),
        in_specs=[pl.BlockSpec(memory_space=pltpu.VMEM)] * count,
        out_specs=[pl.BlockSpec(memory_space=pl.ANY)] * count,
        scratch_shapes=[pltpu.SemaphoreType.DMA((count,))],
        compiler_params=pltpu.CompilerParams(vmem_limit_bytes=1024 * 1024),
        name="emit",
    )(*[pltpu.with_memory_space_constraint(item, pltpu.VMEM) for item in results])


def on_device(
    upstream,
    stream,
    routes,
    route_weights,
    glu_value,
    glu_gate,
    conv_taps,
    conv_saved,
    out_proj,
    expert_gate,
    expert_up,
    expert_down,
):
    tok_count = upstream.shape[0]
    expert_count = lax.axis_size("sp")
    capacity = 4 * tok_count // expert_count
    results = fused(
        expert_count,
        lax.axis_size("tp"),
        capacity,
        routes.T,
        route_weights.T,
        stream,
        upstream,
        expert_gate,
        expert_up,
        expert_down,
        conv_saved,
        out_proj,
        conv_taps,
        glu_value,
        glu_gate,
    )
    return emit(results)


def solution(mesh):
    in_specs = (
        P("sp", None),
        P("sp", None),
        P("sp", None),
        P("sp", None),
        P("sp", "tp"),
        P("sp", "tp"),
        P(None, "tp"),
        P("sp", "tp"),
        P(None, "tp"),
        P("sp", None, "tp"),
        P("sp", None, "tp"),
        P("sp", "tp", None),
    )
    out_specs = (
        P("sp", "tp"),
        P("sp", "tp"),
        P("sp", "tp"),
        P("sp", "tp"),
        P("sp", None, "tp"),
        P("sp", None, "tp"),
        P("sp", "tp", None),
    )
    return jax.shard_map(
        on_device, mesh=mesh, in_specs=in_specs, out_specs=out_specs, check_vma=False
    )
```
